128 devices in a mesh: sp: 16 (over z, y), dp: 8 (over x, core).
Axes of the slice: x: 4, y: 4, z: 4, core: 2. Of those that a mesh axis runs over, the one named last changes fastest.
Arguments:
- stream: bfloat16 [8, 2048, 2048], P('dp', 'sp'), may hold values from -1.796875 to 1.796875
- query_rows: bfloat16 [8, 2048, 2048], P('dp', 'sp'), may hold values from -5 to 5
- key_rows: bfloat16 [8, 2048, 2048], P('dp', 'sp'), may hold values from -5 to 5
- value_rows: bfloat16 [8, 2048, 2048], P('dp', 'sp'), may hold values from -6 to 6
- forget_sums: float32 [8, 16, 2048], P('dp', 'sp'), may hold values from -2048 to 0, as said below
- out_weight: bfloat16 [2048, 2048], replicated, may hold values from -1.5 to 1.5
- first_gain: float32 [2048], replicated, may hold values from 0.1 to 1.9
- expert_ids: int32 [8, 2048, 4], P('dp', 'sp'), may hold values from 0 to 127, all different within a row; in each aligned block of 128 rows (0 to 127, 128 to 255, ..., all dimensions but the last counted through in order) at most 6 rows name the same one
- route_scores: float32 [8, 2048, 4], P('dp', 'sp'), may hold values from -6 to 6
- gate_weight: bfloat16 [128, 2048, 512], P(('sp', 'dp')), may hold values from -0.5 to 0.5
- up_weight: bfloat16 [128, 2048, 512], P(('sp', 'dp')), may hold values from -0.5 to 0.5
- down_weight: bfloat16 [128, 512, 2048], P(('sp', 'dp')), may hold values from -0.0625 to 0.0625
- second_gain: float32 [2048], replicated, may hold values from 0.1 to 1.9
Outputs:
- mixed_stream: bfloat16 [8, 2048, 2048], P('dp', 'sp')
The draws below stay inside these ranges and needn't reach their ends.
Inputs may be any that keep to these rules, and one draw needn't show every extreme that they name: `expert_ids`: each row names 4 different experts; in the rows of one device no expert is named more than 6 times. `forget_sums`: along positions each head's values never rise.
All inputs are finite; a program needn't handle non-finite values.
Results may differ from the reference program's by a relative error of at most 0.0085.
Values may be sent and summed in bfloat16 or wider, within the bound.
No kernel may reach another device: no remote copies, remote signals or barrier semaphores. Data moves between devices by JAX's collectives and lax.ppermute only.
A program may use at most 128 MiB of HBM per device.

```python
import math
import jax
import jax.numpy as jnp
import numpy as np
from jax import lax

D = 2048
HEAD_TOTAL = 16
HD = 128
FF = 512
TOP = 4
TOK_DEV = 128
SEQUENCE_LENGTH = 2048
SEQUENCE_COUNT = 8
EXPERTS = 128
CAP = 6


def draw_query_rows(key, part):
    bulk = jnp.clip(jax.random.normal(jax.random.fold_in(key, 1), (SEQUENCE_COUNT, SEQUENCE_LENGTH, HEAD_TOTAL * HD), jnp.float32), -4.0, 4.0)
    return bulk.astype(jnp.bfloat16)


def draw_key_rows(key, part):
    bulk = jnp.clip(jax.random.normal(jax.random.fold_in(key, 2), (SEQUENCE_COUNT, SEQUENCE_LENGTH, HEAD_TOTAL * HD), jnp.float32), -4.0, 4.0)
    return bulk.astype(jnp.bfloat16)


def draw_forget_sums(key, part):
    key_collection = jax.random.split(jax.random.fold_in(key, 3), 7)
    order = jax.random.permutation(key_collection[0], HEAD_TOTAL)
    fast_count = HEAD_TOTAL // 2
    slow_rate = 0.8 / SEQUENCE_LENGTH * jax.random.uniform(key_collection[1], (HEAD_TOTAL,), jnp.float32, 0.7, 1.4)
    fast_rate = jnp.exp(jax.random.uniform(key_collection[2], (HEAD_TOTAL,), jnp.float32, jnp.log(1.0 / 100.0), jnp.log(1.0 / 30.0)))
    decay_rates = jnp.where(order < fast_count, fast_rate, slow_rate)
    block_count = SEQUENCE_LENGTH // TOK_DEV
    scale_per_block = jnp.exp(jax.random.uniform(key_collection[3], (SEQUENCE_COUNT, 1, block_count), jnp.float32, jnp.log(0.5), jnp.log(2.0)))
    scale_per_block = jnp.repeat(scale_per_block, TOK_DEV, axis=2)
    coarse_estimate = jax.random.uniform(key_collection[4], (SEQUENCE_COUNT, HEAD_TOTAL, SEQUENCE_LENGTH), jnp.float32, 0.3, 1.7)
    surge_position = jax.random.randint(key_collection[5], (SEQUENCE_COUNT, HEAD_TOTAL, 2), 0, SEQUENCE_LENGTH)
    surge_length = jax.random.uniform(key_collection[6], (SEQUENCE_COUNT, HEAD_TOTAL, 2), jnp.float32, 0.22, 0.69)
    position_index = jnp.arange(SEQUENCE_LENGTH, dtype=jnp.int32)
    surge_events = jnp.sum(jnp.where(position_index[None, None, None, :] == surge_position[..., None], surge_length[..., None], 0.0), axis=2)
    gate_logarithms = -decay_rates[None, :, None] * scale_per_block * coarse_estimate - surge_events
    return jnp.cumsum(gate_logarithms, axis=2)


def block_scale(stream_key, extent, cuts, low, top_value):
    level, own = 1.0, jax.random.fold_in(stream_key, 6)
    for axis_at, parts in cuts:
        draws = jnp.exp(jax.random.uniform(jax.random.fold_in(own, axis_at), (parts,), jnp.float32, low / len(cuts), top_value / len(cuts)))
        level = level * jnp.repeat(draws, extent[axis_at] // parts).reshape([-1 if axis == axis_at else 1 for axis in range(len(extent))])
    return level


def routed_block(rng, own, number, rows, amount, top, limit, slope):
    order = jax.random.permutation(rng, amount)
    packed, usual = portions_of(amount, rows * top, limit, slope, True), portions_of(amount, rows * top, limit, slope, False)
    places = jnp.arange(amount)

    def named(tallies, turn):
        used = int((tallies > 0).sum())
        fixed = max(1, used // 4)
        passed = fixed + (places - fixed + turn * (used - fixed)) % max(1, amount - fixed)
        return jnp.zeros((amount,), jnp.int32).at[order[jnp.where(places < fixed, places, passed)]].set(jnp.asarray(tallies, jnp.int32))

    tallies = jnp.where(number % 4 == 0, named(packed, number // 4), named(usual, number - number // 4 - 1))
    mixed = jax.random.permutation(jax.random.fold_in(own, 3), amount)
    source_of, sink = mixed[0:amount // 2 * 2:2], mixed[1:amount // 2 * 2:2]
    slack = jnp.minimum(tallies[source_of] - 1, limit - tallies[sink]) // 2
    slack = jnp.where((source_of == order[0]) | (sink == order[0]) | (tallies[sink] == 0), 0, jnp.maximum(slack, 0))
    passed = jax.random.randint(jax.random.fold_in(own, 4), (amount // 2,), 0, 1 << 20) % (slack + 1)
    tallies = tallies.at[source_of].add(-passed).at[sink].add(passed)
    members = jnp.searchsorted(jnp.cumsum(tallies), jnp.arange(rows * top), side="right").astype(jnp.int32)
    listing = members.reshape(top, rows).T
    listing = listing[jax.random.permutation(jax.random.fold_in(own, 1), rows)]
    turn = jax.random.randint(jax.random.fold_in(own, 2), (rows, 1), 0, top)
    return jnp.take_along_axis(listing, (jnp.arange(top)[None, :] + turn) % top, axis=1)


def portions_of(amount, total, reach, lean, full):
    weights = [(1 << 20) // math.isqrt(grade ** lean) + 1 for grade in range(1, amount + 1)]
    largest = reach if full else min(reach, max(-(-total // amount), total * weights[0] // sum(weights)))
    least = 1 if total - largest >= amount - 1 else 0
    counts, spare = [largest] + [least] * (amount - 1), total - largest - least * (amount - 1)
    while spare > 0:
        movable = [i for i in range(1, amount) if counts[i] < largest] or [i for i in range(1, amount) if counts[i] < reach]
        whole, budget = sum([weights[i] for i in movable]), spare
        for i in movable:
            more = min(reach - counts[i], max(1, budget * weights[i] // whole), spare)
            counts[i] = counts[i] + more
            spare = spare - more
    return np.array(counts)


def bell_draw(own_key, dims, deviation, limit, cuts=(), held_as=jnp.bfloat16):
    entries = jax.random.normal(own_key, dims, jnp.float32) * deviation
    if len(cuts) > 0:
        entries = block_scale(own_key, dims, cuts, -0.22, 0.18) * entries
    return jnp.clip(entries, min=-limit, max=limit).astype(held_as)


def setup_inputs(seed: int = 0) -> dict:
    key_of = jax.random.split(jax.random.key(seed), 14)
    stream = bell_draw(key_of[0], (SEQUENCE_COUNT, SEQUENCE_LENGTH, D), 0.3, 1.796875, ((0, 8), (1, 16)))
    query_rows = draw_query_rows(jax.random.fold_in(key_of[13], 71), 0)
    key_rows = draw_key_rows(jax.random.fold_in(key_of[13], 71), 0)
    value_rows = bell_draw(key_of[3], (SEQUENCE_COUNT, SEQUENCE_LENGTH, HEAD_TOTAL * HD), 1.0, 6.0, ((0, 8), (1, 16)))
    forget_sums = draw_forget_sums(jax.random.fold_in(key_of[13], 71), 0)
    out_weight = bell_draw(key_of[5], (HEAD_TOTAL * HD, D), (HD // 8) ** -0.5, 1.5)
    first_gain = jnp.clip(1.0 + 0.18 * jax.random.normal(key_of[6], (D,), jnp.float32), 0.1, 1.9)
    expert_ids_keys = jax.random.split(jax.random.fold_in(key_of[7], 1), SEQUENCE_COUNT * SEQUENCE_LENGTH // TOK_DEV)
    expert_ids_turns = jax.random.permutation(jax.random.fold_in(key_of[7], 3), SEQUENCE_COUNT * SEQUENCE_LENGTH // TOK_DEV)
    expert_ids = jax.vmap(lambda own, number: routed_block(jax.random.fold_in(key_of[7], 2), own, number, TOK_DEV, EXPERTS, TOP, CAP, 2))(expert_ids_keys, expert_ids_turns).reshape((SEQUENCE_COUNT, SEQUENCE_LENGTH, TOP))
    route_scores = bell_draw(key_of[8], (SEQUENCE_COUNT, SEQUENCE_LENGTH, TOP), 1.0, 6.0, ((0, 8), (1, 16)), jnp.float32)
    gate_weight = bell_draw(key_of[9], (EXPERTS, D, FF), (D // 16) ** -0.5, 0.5, ((0, 128),))
    up_weight = bell_draw(key_of[10], (EXPERTS, D, FF), (D // 16) ** -0.5, 0.5, ((0, 128),))
    down_weight = bell_draw(key_of[11], (EXPERTS, FF, D), (16 * FF) ** -0.5, 0.0625, ((0, 128),))
    second_gain = jnp.clip(1.0 + 0.18 * jax.random.normal(key_of[12], (D,), jnp.float32), 0.1, 1.9)
    return dict(stream=stream, query_rows=query_rows, key_rows=key_rows, value_rows=value_rows, forget_sums=forget_sums, out_weight=out_weight, first_gain=first_gain, expert_ids=expert_ids, route_scores=route_scores, gate_weight=gate_weight, up_weight=up_weight, down_weight=down_weight, second_gain=second_gain)


deep_alpha = 8.0 ** 0.25
clamp_limit = 7.0
swish_alpha = 1.702
norm_eps = 1e-05
mask_fill = -1e+30

def layer_norm(summed, gain_row):
    centre = lax.optimization_barrier(jnp.mean(summed, axis=-1, keepdims=True))
    spread = lax.optimization_barrier(jnp.mean(jnp.square(summed - centre), axis=-1, keepdims=True))
    return (summed - centre) * lax.rsqrt(spread + norm_eps) * gain_row

def attend_head(query_head, key_head, value_head, gate_head):
    length = query_head.shape[0]
    q_block = min(512, length)
    block_count = length // q_block
    inv_root = query_head.shape[1] ** (-0.5)
    key_pos = jnp.arange(length, dtype=jnp.int32)

    def one_block(block_index):
        first_row = block_index * q_block
        row_block = lax.dynamic_slice_in_dim(query_head, first_row, q_block, 0)
        row_gate = lax.dynamic_slice_in_dim(gate_head, first_row, q_block, 0)
        scores = jnp.dot(row_block, key_head.T, preferred_element_type=jnp.float32) * inv_root
        scores = scores + row_gate[:, None] - gate_head[None, :]
        query_pos = first_row + jnp.arange(q_block, dtype=jnp.int32)
        scores = jnp.where(query_pos[:, None] >= key_pos[None, :], scores, mask_fill)
        row_max = lax.optimization_barrier(jnp.max(scores, axis=1, keepdims=True))
        weights = jnp.exp(scores - row_max)
        row_total = lax.optimization_barrier(jnp.sum(weights, axis=1, keepdims=True))
        blended = jnp.dot(weights.astype(jnp.bfloat16), value_head, preferred_element_type=jnp.float32)
        return (blended / row_total).astype(jnp.bfloat16)
    return lax.map(one_block, jnp.arange(block_count, dtype=jnp.int32)).reshape(length, -1)

def expert_rows(row_block, gate_matrix, up_matrix, down_matrix):
    gate_act = jnp.minimum(jnp.dot(row_block, gate_matrix, preferred_element_type=jnp.float32), clamp_limit)
    up_act = jnp.clip(jnp.dot(row_block, up_matrix, preferred_element_type=jnp.float32), -clamp_limit, clamp_limit)
    hidden = (gate_act * jax.nn.sigmoid(swish_alpha * gate_act) * (up_act + 1.0)).astype(jnp.bfloat16)
    return jnp.dot(hidden, down_matrix, preferred_element_type=jnp.float32).astype(jnp.bfloat16)

def reference(stream, query_rows, key_rows, value_rows, forget_sums, out_weight, first_gain, expert_ids, route_scores, gate_weight, up_weight, down_weight, second_gain):

    def split_heads(head_rows):
        return head_rows.reshape(SEQUENCE_COUNT, SEQUENCE_LENGTH, HEAD_TOTAL, HD).transpose(0, 2, 1, 3).reshape(SEQUENCE_COUNT * HEAD_TOTAL, SEQUENCE_LENGTH, HD)
    attended = lax.map(lambda head_parts: attend_head(head_parts[0], head_parts[1], head_parts[2], head_parts[3]), (split_heads(query_rows), split_heads(key_rows), split_heads(value_rows), forget_sums.reshape(SEQUENCE_COUNT * HEAD_TOTAL, SEQUENCE_LENGTH)))
    attended = attended.reshape(SEQUENCE_COUNT, HEAD_TOTAL, SEQUENCE_LENGTH, HD).transpose(0, 2, 1, 3).reshape(SEQUENCE_COUNT * SEQUENCE_LENGTH, HEAD_TOTAL * HD)
    projected = jnp.dot(attended, out_weight, preferred_element_type=jnp.float32)
    summed = deep_alpha * stream.reshape(SEQUENCE_COUNT * SEQUENCE_LENGTH, D).astype(jnp.float32) + projected
    first_stream = layer_norm(summed, first_gain).astype(jnp.bfloat16)
    flat_ids = expert_ids.reshape(-1).astype(jnp.int32)
    route_weights = jax.nn.softmax(route_scores.reshape(-1, TOP), axis=-1).reshape(-1)
    most_rows = CAP * (SEQUENCE_COUNT * SEQUENCE_LENGTH // TOK_DEV)

    def expert_step(running, inputs):
        gate_matrix, up_matrix, down_matrix, expert_index = inputs
        chosen = flat_ids == expert_index
        picked = jnp.nonzero(chosen, size=most_rows, fill_value=0)[0].astype(jnp.int32)
        is_valid = (jnp.arange(most_rows, dtype=jnp.int32) < jnp.sum(chosen.astype(jnp.int32))).astype(jnp.float32)
        token_index = picked // TOP
        outputs = expert_rows(first_stream[token_index], gate_matrix, up_matrix, down_matrix)
        scaled = outputs.astype(jnp.float32) * (route_weights[picked] * is_valid)[:, None]
        return (running.at[token_index].add(scaled), None)
    mixture, _ = lax.scan(expert_step, jnp.zeros((SEQUENCE_COUNT * SEQUENCE_LENGTH, D), jnp.float32), (gate_weight, up_weight, down_weight, jnp.arange(EXPERTS, dtype=jnp.int32)))
    second = layer_norm(deep_alpha * first_stream.astype(jnp.float32) + mixture, second_gain)
    return second.astype(jnp.bfloat16).reshape(SEQUENCE_COUNT, SEQUENCE_LENGTH, D)
```

```python
import jax
import jax.numpy as jnp
from jax import lax
from jax.experimental import pallas as pl
from jax.experimental.pallas import tpu as pltpu
from jax.sharding import Mesh
from jax.sharding import PartitionSpec as P

SP = ("sp_0", "sp_1")
SP_DP = ("sp_0", "sp_1", "dp")

deep_alpha = 8.0**0.25
clamp_limit = 7.0
swish_alpha = 1.702
norm_eps = 1e-05
mask_fill = -1e30
log2_e = 1.4426950408889634

LANE = 128
SUB = 8
SLOTS = 6
MAIN = 12
TAIL = 4
MIB = 1 << 20


def call(body, out_shape, vmem_mib, **kwargs):
    return pl.pallas_call(
        body,
        out_shape=out_shape,
        compiler_params=pltpu.CompilerParams(vmem_limit_bytes=vmem_mib * MIB),
        **kwargs,
    )


def dot(a, b, dims=((1,), (0,))):
    return lax.dot_general(a, b, (dims, ((), ())), preferred_element_type=jnp.float32)


def layer_norm(summed, gain_row):
    centre = jnp.mean(summed, axis=-1, keepdims=True)
    centred = summed - centre
    spread = jnp.mean(jnp.square(centred), axis=-1, keepdims=True)
    return centred * lax.rsqrt(spread + norm_eps) * gain_row


def pack_heads_body(q_ref, k_ref, v_ref, out_ref):
    for h in range(out_ref.shape[0]):
        for n, ref in enumerate((q_ref, k_ref, v_ref)):
            out_ref[h, n] = ref[0, :, h * LANE : (h + 1) * LANE]


def pack_heads(q, k, v):
    rows, width = q.shape[1:]
    heads, step = width // LANE, 4
    spec = pl.BlockSpec((1, rows, step * LANE), lambda i: (0, 0, i))
    return call(
        pack_heads_body,
        jax.ShapeDtypeStruct((heads, 3, rows, LANE), q.dtype),
        16,
        grid=(heads // step,),
        in_specs=[spec] * 3,
        out_specs=pl.BlockSpec((step, 3, rows, LANE), lambda i: (i, 0, 0, 0)),
    )(q, k, v)


def attend_body(qkv_ref, gate_ref, out_ref, score_ref):
    parts, _, rows, size = qkv_ref.shape
    pair = 2
    block = pair * rows
    scale = size ** (-0.5) * log2_e
    for b in range(parts // pair):
        q = qkv_ref[pair * b : pair * (b + 1), 0].reshape(block, size)
        base = gate_ref[:, block * b : block * b + 1]
        top = jnp.full((block, LANE), mask_fill, jnp.float32)
        for j in range(b + 1):
            keys = qkv_ref[pair * j : pair * (j + 1), 1].reshape(block, size)
            bias = (gate_ref[:, block * j : block * (j + 1)] - base) * log2_e
            s = dot(q, keys, ((1,), (1,))) * scale - bias
            if j == b:
                row = lax.broadcasted_iota(jnp.int32, s.shape, 0)
                col = lax.broadcasted_iota(jnp.int32, s.shape, 1)
                s = jnp.where(row >= col, s, mask_fill)
            score_ref[:, block * j : block * (j + 1)] = s
            for c in range(block // LANE):
                top = jnp.maximum(top, s[:, c * LANE : (c + 1) * LANE])
        row_max = jnp.max(top, axis=1, keepdims=True)
        total = jnp.zeros((block, LANE), jnp.float32)
        blended = jnp.zeros((block, size), jnp.float32)
        for j in range(b + 1):
            w = jnp.exp2(score_ref[:, block * j : block * (j + 1)] - row_max)
            for c in range(block // LANE):
                total = total + w[:, c * LANE : (c + 1) * LANE]
            values = qkv_ref[pair * j : pair * (j + 1), 2].reshape(block, size)
            blended = blended + dot(w.astype(jnp.bfloat16), values)
        row_total = jnp.sum(total, axis=1, keepdims=True)
        done = (blended / row_total).astype(jnp.bfloat16)
        out_ref[pair * b : pair * (b + 1)] = done.reshape(pair, rows, size)


def attend(qkv, gates):
    parts, _, rows, size = qkv.shape
    return call(
        attend_body,
        jax.ShapeDtypeStruct((parts, rows, size), qkv.dtype),
        24,
        scratch_shapes=[pltpu.VMEM((2 * rows, parts * rows), jnp.float32)],
    )(qkv, gates)


def slot_of(place, kind):
    if kind == 0:
        return jnp.where(place < SLOTS, place, -2)
    return jnp.where(place >= SLOTS, place - SLOTS + 2 * (kind - 1), -2)


def route_body(ids_ref, score_ref, pick_ref, blend_ref):
    rows, top_k = ids_ref.shape[1:]
    experts = pick_ref.shape[1] // SUB
    expert = lax.broadcasted_iota(jnp.int32, (rows, experts), 1)
    scores = score_ref[0]
    raised = jnp.exp(scores - jnp.max(scores, axis=1, keepdims=True))
    shares = raised / jnp.sum(raised, axis=1, keepdims=True)
    named = jnp.zeros((rows, experts), jnp.float32)
    share = jnp.zeros((rows, experts), jnp.float32)
    for k in range(top_k):
        hit = ids_ref[0, :, k : k + 1] == expert
        named = jnp.where(hit, 1.0, named)
        share = jnp.where(hit, shares[:, k : k + 1], share)
    earlier = lax.broadcasted_iota(jnp.int32, (rows, rows), 0) > lax.broadcasted_iota(
        jnp.int32, (rows, rows), 1
    )
    rank = dot(jnp.where(earlier, 1.0, 0.0).astype(jnp.bfloat16), named.astype(jnp.bfloat16))
    slot = jnp.where(named > 0.0, rank, -1.0)
    by_expert = jnp.broadcast_to(slot.T[:, None, :], (experts, SUB, rows))
    place = lax.broadcasted_iota(jnp.int32, (experts, SUB, rows), 1)
    for kind in range(4):
        hit = by_expert == slot_of(place, kind).astype(jnp.float32)
        pick = jnp.where(hit, 1.0, 0.0).reshape(experts * SUB, rows).astype(jnp.bfloat16)
        pick_ref[kind] = pick
    wide = (experts, experts * SUB)
    spread = lax.broadcasted_iota(jnp.int32, wide, 0) == lax.broadcasted_iota(
        jnp.int32, wide, 1
    ) // SUB
    spread = jnp.where(spread, 1.0, 0.0).astype(jnp.bfloat16)
    wide_slot = dot(slot.astype(jnp.bfloat16), spread)
    wide_share = dot(share.astype(jnp.bfloat16), spread)
    place = lax.broadcasted_iota(jnp.int32, wide_slot.shape, 1) % SUB
    for kind in range(4):
        hit = wide_slot == slot_of(place, kind).astype(jnp.float32)
        blend_ref[kind] = jnp.where(hit, wide_share, 0.0).astype(jnp.bfloat16)


def route(ids, scores, experts):
    rows = ids.shape[1]
    return call(
        route_body,
        (
            jax.ShapeDtypeStruct((4, experts * SUB, rows), jnp.bfloat16),
            jax.ShapeDtypeStruct((4, rows, experts * SUB), jnp.bfloat16),
        ),
        24,
    )(ids, scores)


def project_body(heads_ref, stream_ref, weight_ref, gain_ref, pick_ref, first_ref, out_ref):
    heads = heads_ref.shape[0]
    experts = out_ref.shape[0]
    attended = jnp.concatenate([heads_ref[h] for h in range(heads)], axis=1)
    projected = dot(attended, weight_ref[...])
    summed = deep_alpha * stream_ref[0].astype(jnp.float32) + projected
    first = layer_norm(summed, gain_ref[...]).astype(jnp.bfloat16)
    first_ref[...] = first
    tail = first[:, MAIN * LANE :]
    for p in range(3):
        kept = [first[:, (3 * q + p) * LANE : (3 * q + p + 1) * LANE] for q in range(TAIL)]
        both = jnp.concatenate([jnp.concatenate(kept, axis=1), tail], axis=0)
        lhs = jnp.concatenate([pick_ref[0], pick_ref[p + 1]], axis=1)
        rows = dot(lhs, both).astype(jnp.bfloat16)
        for q in range(TAIL):
            tile = rows[:, q * LANE : (q + 1) * LANE]
            out_ref[:, 3 * q + p] = tile.reshape(experts, SUB, LANE)


def project(heads, stream, weight, gain, pick):
    rows, width = stream.shape[1:]
    experts = pick.shape[1] // SUB
    return call(
        project_body,
        (
            jax.ShapeDtypeStruct((rows, width), jnp.bfloat16),
            jax.ShapeDtypeStruct((experts, MAIN, SUB, LANE), jnp.bfloat16),
        ),
        36,
    )(heads, stream, weight, gain, pick)


def move_matrix(rows, p):
    to = lax.broadcasted_iota(jnp.int32, (rows, rows), 0)
    fro = lax.broadcasted_iota(jnp.int32, (rows, rows), 1)
    same = to // SUB == fro // SUB
    hit = same & (fro % SUB - SLOTS + 2 * p == to % SUB) & (fro % SUB >= SLOTS)
    return jnp.where(hit, 1.0, 0.0).astype(jnp.bfloat16)


def expert_body(in_ref, gate_ref, up_ref, down_ref, out_ref):
    sources = in_ref.shape[0]
    rows = sources * SUB
    kept = [in_ref[:, t].reshape(rows, LANE) for t in range(MAIN)]
    tail = jnp.zeros((rows, TAIL * LANE), jnp.float32)
    for p in range(3):
        spare = jnp.concatenate([kept[3 * q + p] for q in range(TAIL)], axis=1)
        tail = tail + dot(move_matrix(rows, p), spare)
    x = jnp.concatenate(kept + [tail.astype(jnp.bfloat16)], axis=1)
    gate_act = jnp.minimum(dot(x, gate_ref[0]), clamp_limit)
    up_act = jnp.clip(dot(x, up_ref[0]), -clamp_limit, clamp_limit)
    hidden = gate_act * jax.nn.sigmoid(swish_alpha * gate_act) * (up_act + 1.0)
    y = dot(hidden.astype(jnp.bfloat16), down_ref[0])
    y_tail = y[:, MAIN * LANE :].astype(jnp.bfloat16)
    own = lax.broadcasted_iota(jnp.int32, (rows, LANE), 0) % SUB < SLOTS
    for p in range(3):
        spare = dot(move_matrix(rows, p), y_tail, ((0,), (0,)))
        for q in range(TAIL):
            t = 3 * q + p
            tile = jnp.where(
                own, y[:, t * LANE : (t + 1) * LANE], spare[:, q * LANE : (q + 1) * LANE]
            )
            out_ref[:, t] = tile.astype(jnp.bfloat16).reshape(sources, SUB, LANE)


def expert(arrived, gate, up, down):
    sources, step = arrived.shape[0], 32
    block = pl.BlockSpec((step, MAIN, SUB, LANE), lambda i: (i, 0, 0, 0))
    whole = [pl.BlockSpec(w.shape, lambda i: (0, 0, 0)) for w in (gate, up, down)]
    return call(
        expert_body,
        jax.ShapeDtypeStruct(arrived.shape, arrived.dtype),
        36,
        grid=(sources // step,),
        in_specs=[block] + whole,
        out_specs=block,
    )(arrived, gate, up, down)


def combine_body(in_ref, blend_ref, first_ref, gain_ref, out_ref):
    experts = in_ref.shape[0]
    tail = None
    blocks = [None] * MAIN
    for p in range(3):
        rows = [in_ref[:, 3 * q + p].reshape(experts * SUB, LANE) for q in range(TAIL)]
        both = jnp.concatenate([blend_ref[0], blend_ref[p + 1]], axis=0)
        mixed = dot(both, jnp.concatenate(rows, axis=1))
        count = blend_ref.shape[1]
        for q in range(TAIL):
            blocks[3 * q + p] = mixed[:count, q * LANE : (q + 1) * LANE]
        tail = mixed[count:] if tail is None else tail + mixed[count:]
    mixture = jnp.concatenate(blocks + [tail], axis=1)
    summed = deep_alpha * first_ref[...].astype(jnp.float32) + mixture
    out_ref[0] = layer_norm(summed, gain_ref[...]).astype(jnp.bfloat16)


def combine(returned, blend, first, gain):
    return call(
        combine_body,
        jax.ShapeDtypeStruct((1, *first.shape), jnp.bfloat16),
        36,
    )(returned, blend, first, gain)


def exchange(x, axes):
    return lax.all_to_all(x, axes, split_axis=0, concat_axis=0, tiled=True)


def shards(
    stream,
    query_rows,
    key_rows,
    value_rows,
    forget_sums,
    out_weight,
    first_gain,
    expert_ids,
    route_scores,
    gate_weight,
    up_weight,
    down_weight,
    second_gain,
):
    experts = lax.axis_size(SP_DP)
    qkv = exchange(pack_heads(query_rows, key_rows, value_rows), SP)
    pick, blend = route(expert_ids, route_scores, experts)
    heads = exchange(attend(qkv, forget_sums[0]), SP)
    first, outgoing = project(heads, stream, out_weight, first_gain[None], pick)
    arrived = exchange(outgoing, SP_DP)
    finished = expert(arrived, gate_weight, up_weight, down_weight)
    returned = exchange(finished, SP_DP)
    return combine(returned, blend, first, second_gain[None])


def solution(mesh):
    finer = Mesh(mesh.devices.reshape(4, 4, mesh.shape["dp"]), ("sp_0", "sp_1", "dp"))
    rows = P("dp", SP, None)
    own = P(SP_DP, None, None)
    placed = (rows,) * 5 + (P(), P(), rows, rows, own, own, own, P())
    return jax.shard_map(shards, mesh=finer, in_specs=placed, out_specs=rows, check_vma=False)
```

```python
import jax
import jax.numpy as jnp
from jax import lax
from jax.experimental import pallas as pl
from jax.experimental.pallas import tpu as pltpu
from jax.sharding import Mesh
from jax.sharding import PartitionSpec as P

SP = ("sp_0", "sp_1")
SP_DP = ("sp_0", "sp_1", "dp")

deep_alpha = 8.0**0.25
clamp_limit = 7.0
swish_alpha = 1.702
norm_eps = 1e-05
mask_fill = -1e30
log2_e = 1.4426950408889634

LANE = 128
SUB = 8
SLOTS = 6
MAIN = 12
TAIL = 4
MIB = 1 << 20


def call(body, out_shape, vmem_mib, **kwargs):
    return pl.pallas_call(
        body,
        out_shape=out_shape,
        compiler_params=pltpu.CompilerParams(vmem_limit_bytes=vmem_mib * MIB),
        **kwargs,
    )


def dot(a, b, dims=((1,), (0,))):
    return lax.dot_general(a, b, (dims, ((), ())), preferred_element_type=jnp.float32)


def layer_norm(summed, gain_row):
    centre = jnp.mean(summed, axis=-1, keepdims=True)
    centred = summed - centre
    spread = jnp.mean(jnp.square(centred), axis=-1, keepdims=True)
    return centred * lax.rsqrt(spread + norm_eps) * gain_row


def in_hbm(*arrays):
    return tuple(pltpu.with_memory_space_constraint(a, pltpu.HBM) for a in arrays)


def slot_of(place, kind):
    if kind == 0:
        return jnp.where(place < SLOTS, place, -2)
    return jnp.where(place >= SLOTS, place - SLOTS + 2 * (kind - 1), -2)


def prepare_body(
    q_ref, k_ref, v_ref, ids_hbm, score_hbm, out_ref, pick_ref, blend_ref, ids_ref, score_ref, sems, small
):
    lists = [
        pltpu.make_async_copy(ids_hbm, ids_ref, small.at[0]),
        pltpu.make_async_copy(score_hbm, score_ref, small.at[1]),
    ]
    copies = []
    for h in range(out_ref.shape[0]):
        for n, ref in enumerate((q_ref, k_ref, v_ref)):
            source = ref.at[0, :, h * LANE : (h + 1) * LANE]
            copies.append(pltpu.make_async_copy(source, out_ref.at[h, n], sems.at[h, n]))
    for copy in lists + copies:
        copy.start()
    for copy in lists:
        copy.wait()
    top_k, rows = ids_ref.shape[1:]
    experts = pick_ref.shape[1] // SUB
    expert = lax.broadcasted_iota(jnp.int32, (experts, rows), 0)
    scores = score_ref[0]
    raised = jnp.exp(scores - jnp.max(scores, axis=0, keepdims=True))
    shares = raised / jnp.sum(raised, axis=0, keepdims=True)
    named = jnp.zeros((experts, rows), jnp.float32)
    share = jnp.zeros((experts, rows), jnp.float32)
    for k in range(top_k):
        hit = ids_ref[0, k : k + 1] == expert
        named = jnp.where(hit, 1.0, named)
        share = jnp.where(hit, shares[k : k + 1], share)
    earlier = lax.broadcasted_iota(jnp.int32, (rows, rows), 0) < lax.broadcasted_iota(
        jnp.int32, (rows, rows), 1
    )
    rank = dot(named.astype(jnp.bfloat16), jnp.where(earlier, 1.0, 0.0).astype(jnp.bfloat16))
    slot = jnp.where(named > 0.0, rank, -1.0)
    by_expert = jnp.broadcast_to(slot[:, None, :], (experts, SUB, rows))
    place = lax.broadcasted_iota(jnp.int32, (experts, SUB, rows), 1)
    for kind in range(4):
        hit = by_expert == slot_of(place, kind).astype(jnp.float32)
        pick = jnp.where(hit, 1.0, 0.0).reshape(experts * SUB, rows).astype(jnp.bfloat16)
        pick_ref[kind] = pick
    wide = (experts, experts * SUB)
    spread = lax.broadcasted_iota(jnp.int32, wide, 0) == lax.broadcasted_iota(
        jnp.int32, wide, 1
    ) // SUB
    spread = jnp.where(spread, 1.0, 0.0).astype(jnp.bfloat16)
    wide_slot = dot(slot.T.astype(jnp.bfloat16), spread)
    wide_share = dot(share.T.astype(jnp.bfloat16), spread)
    place = lax.broadcasted_iota(jnp.int32, wide_slot.shape, 1) % SUB
    for kind in range(4):
        hit = wide_slot == slot_of(place, kind).astype(jnp.float32)
        blend_ref[kind] = jnp.where(hit, wide_share, 0.0).astype(jnp.bfloat16)
    for copy in copies:
        copy.wait()


def prepare(q, k, v, ids, scores, experts):
    rows, width = q.shape[1:]
    heads = width // LANE
    near = pl.BlockSpec(memory_space=pltpu.VMEM)
    return call(
        prepare_body,
        (
            pltpu.VMEM((heads, 3, rows, LANE), q.dtype),
            jax.ShapeDtypeStruct((4, experts * SUB, rows), jnp.bfloat16),
            jax.ShapeDtypeStruct((4, rows, experts * SUB), jnp.bfloat16),
        ),
        16,
        in_specs=[pl.BlockSpec(memory_space=pltpu.HBM)] * 5,
        out_specs=(near,) * 3,
        scratch_shapes=[
            pltpu.VMEM(ids.shape, ids.dtype),
            pltpu.VMEM(scores.shape, scores.dtype),
            pltpu.SemaphoreType.DMA((heads, 3)),
            pltpu.SemaphoreType.DMA((2,)),
        ],
    )(*in_hbm(q, k, v, ids, scores))


def attend_body(qkv_ref, gate_ref, weight_ref, out_ref, near_ref, score_ref, sem):
    brought = pltpu.make_async_copy(weight_ref, near_ref, sem)
    brought.start()
    parts, _, rows, size = qkv_ref.shape
    pair = 2
    block = pair * rows
    scale = size ** (-0.5) * log2_e
    for b in range(parts // pair):
        q = qkv_ref[pair * b : pair * (b + 1), 0].reshape(block, size)
        base = gate_ref[:, block * b : block * b + 1]
        top = jnp.full((block, LANE), mask_fill, jnp.float32)
        for j in range(b + 1):
            keys = qkv_ref[pair * j : pair * (j + 1), 1].reshape(block, size)
            bias = (gate_ref[:, block * j : block * (j + 1)] - base) * log2_e
            s = dot(q, keys, ((1,), (1,))) * scale - bias
            if j == b:
                row = lax.broadcasted_iota(jnp.int32, s.shape, 0)
                col = lax.broadcasted_iota(jnp.int32, s.shape, 1)
                s = jnp.where(row >= col, s, mask_fill)
            score_ref[:, block * j : block * (j + 1)] = s
            for c in range(block // LANE):
                top = jnp.maximum(top, s[:, c * LANE : (c + 1) * LANE])
        row_max = jnp.max(top, axis=1, keepdims=True)
        total = jnp.zeros((block, LANE), jnp.float32)
        blended = jnp.zeros((block, size), jnp.float32)
        for j in range(b + 1):
            w = jnp.exp2(score_ref[:, block * j : block * (j + 1)] - row_max)
            for c in range(block // LANE):
                total = total + w[:, c * LANE : (c + 1) * LANE]
            values = qkv_ref[pair * j : pair * (j + 1), 2].reshape(block, size)
            blended = blended + dot(w.astype(jnp.bfloat16), values)
        row_total = jnp.sum(total, axis=1, keepdims=True)
        done = (blended / row_total).astype(jnp.bfloat16)
        out_ref[pair * b : pair * (b + 1)] = done.reshape(pair, rows, size)
    brought.wait()


def attend(qkv, gates, weight):
    parts, _, rows, size = qkv.shape
    near = pl.BlockSpec(memory_space=pltpu.VMEM)
    return call(
        attend_body,
        (
            jax.ShapeDtypeStruct((parts, rows, size), qkv.dtype),
            pltpu.VMEM(weight.shape, weight.dtype),
        ),
        20,
        in_specs=[near, near, pl.BlockSpec(memory_space=pltpu.HBM)],
        out_specs=(near, near),
        scratch_shapes=[
            pltpu.VMEM((2 * rows, parts * rows), jnp.float32),
            pltpu.SemaphoreType.DMA,
        ],
    )(qkv, gates, *in_hbm(weight))


def project_body(heads_ref, stream_ref, weight_ref, gain_ref, pick_ref, first_ref, out_ref):
    heads = heads_ref.shape[0]
    experts = out_ref.shape[0]
    attended = jnp.concatenate([heads_ref[h] for h in range(heads)], axis=1)
    projected = dot(attended, weight_ref[...])
    summed = deep_alpha * stream_ref[0].astype(jnp.float32) + projected
    first = layer_norm(summed, gain_ref[...]).astype(jnp.bfloat16)
    first_ref[...] = first
    tail = first[:, MAIN * LANE :]
    for p in range(3):
        kept = [first[:, (3 * q + p) * LANE : (3 * q + p + 1) * LANE] for q in range(TAIL)]
        both = jnp.concatenate([jnp.concatenate(kept, axis=1), tail], axis=0)
        lhs = jnp.concatenate([pick_ref[0], pick_ref[p + 1]], axis=1)
        rows = dot(lhs, both).astype(jnp.bfloat16)
        for q in range(TAIL):
            tile = rows[:, q * LANE : (q + 1) * LANE]
            out_ref[:, 3 * q + p] = tile.reshape(experts, SUB, LANE)


def project(heads, stream, weight, gain, pick):
    rows, width = stream.shape[1:]
    experts = pick.shape[1] // SUB
    return call(
        project_body,
        (
            jax.ShapeDtypeStruct((rows, width), jnp.bfloat16),
            jax.ShapeDtypeStruct((experts, MAIN, SUB, LANE), jnp.bfloat16),
        ),
        36,
    )(heads, stream, weight, gain, pick)


def expert_body(in_ref, gate_ref, up_ref, down_ref, out_ref):
    sources = in_ref.shape[0]
    rows = sources * SUB
    place = lax.broadcasted_iota(jnp.int32, (rows, LANE), 0) % SUB
    kept = [in_ref[:, t].reshape(rows, LANE) for t in range(MAIN)]
    tail = []
    for q in range(TAIL):
        spare = [
            pltpu.roll(kept[3 * q + p].astype(jnp.float32), rows - SLOTS + 2 * p, 0)
            for p in range(3)
        ]
        block = jnp.where(place < 2, spare[0], jnp.where(place < 4, spare[1], spare[2]))
        tail.append(block.astype(jnp.bfloat16))
    x = jnp.concatenate(kept + tail, axis=1)
    gate_act = jnp.minimum(dot(x, gate_ref[0]), clamp_limit)
    up_act = jnp.clip(dot(x, up_ref[0]), -clamp_limit, clamp_limit)
    hidden = gate_act * jax.nn.sigmoid(swish_alpha * gate_act) * (up_act + 1.0)
    y = dot(hidden.astype(jnp.bfloat16), down_ref[0])
    for t in range(MAIN):
        q, p = t // 3, t % 3
        spare = pltpu.roll(y[:, (MAIN + q) * LANE : (MAIN + q + 1) * LANE], SLOTS - 2 * p, 0)
        tile = jnp.where(place < SLOTS, y[:, t * LANE : (t + 1) * LANE], spare)
        out_ref[:, t] = tile.astype(jnp.bfloat16).reshape(sources, SUB, LANE)


def expert(arrived, gate, up, down):
    sources, step = arrived.shape[0], 64
    block = pl.BlockSpec((step, MAIN, SUB, LANE), lambda i: (i, 0, 0, 0))
    whole = [pl.BlockSpec(w.shape, lambda i: (0, 0, 0)) for w in (gate, up, down)]
    return call(
        expert_body,
        jax.ShapeDtypeStruct(arrived.shape, arrived.dtype),
        36,
        grid=(sources // step,),
        in_specs=[block] + whole,
        out_specs=block,
    )(arrived, gate, up, down)


def combine_body(in_ref, blend_ref, first_ref, gain_ref, out_ref):
    experts = in_ref.shape[0]
    tail = None
    blocks = [None] * MAIN
    for p in range(3):
        rows = [in_ref[:, 3 * q + p].reshape(experts * SUB, LANE) for q in range(TAIL)]
        both = jnp.concatenate([blend_ref[0], blend_ref[p + 1]], axis=0)
        mixed = dot(both, jnp.concatenate(rows, axis=1))
        count = blend_ref.shape[1]
        for q in range(TAIL):
            blocks[3 * q + p] = mixed[:count, q * LANE : (q + 1) * LANE]
        tail = mixed[count:] if tail is None else tail + mixed[count:]
    mixture = jnp.concatenate(blocks + [tail], axis=1)
    summed = deep_alpha * first_ref[...].astype(jnp.float32) + mixture
    out_ref[0] = layer_norm(summed, gain_ref[...]).astype(jnp.bfloat16)


def combine(returned, blend, first, gain):
    return call(
        combine_body,
        jax.ShapeDtypeStruct((1, *first.shape), jnp.bfloat16),
        36,
    )(returned, blend, first, gain)


def exchange(x, axes):
    return lax.all_to_all(x, axes, split_axis=0, concat_axis=0, tiled=True)


def shards(
    stream,
    query_rows,
    key_rows,
    value_rows,
    forget_sums,
    out_weight,
    first_gain,
    expert_ids,
    route_scores,
    gate_weight,
    up_weight,
    down_weight,
    second_gain,
):
    experts = lax.axis_size(SP_DP)
    packed, pick, blend = prepare(
        query_rows,
        key_rows,
        value_rows,
        expert_ids.transpose(0, 2, 1),
        route_scores.transpose(0, 2, 1),
        experts,
    )
    qkv = exchange(packed, SP)
    attended, near_weight = attend(qkv, forget_sums[0], out_weight)
    heads = exchange(attended, SP)
    first, outgoing = project(heads, stream, near_weight, first_gain[None], pick)
    arrived = exchange(outgoing, SP_DP)
    finished = expert(arrived, gate_weight, up_weight, down_weight)
    returned = exchange(finished, SP_DP)
    return combine(returned, blend, first, second_gain[None])


def solution(mesh):
    finer = Mesh(mesh.devices.reshape(4, 4, mesh.shape["dp"]), ("sp_0", "sp_1", "dp"))
    rows = P("dp", SP, None)
    own = P(SP_DP, None, None)
    placed = (rows,) * 5 + (P(), P(), rows, rows, own, own, own, P())
    return jax.shard_map(shards, mesh=finer, in_specs=placed, out_specs=rows, check_vma=False)
```

```python
import jax
import jax.numpy as jnp
from jax import lax
from jax.experimental import pallas as pl
from jax.experimental.pallas import tpu as pltpu
from jax.sharding import Mesh
from jax.sharding import PartitionSpec as P

SP = ("sp_0", "sp_1")
SP_DP = ("sp_0", "sp_1", "dp")

deep_alpha = 8.0**0.25
clamp_limit = 7.0
swish_alpha = 1.702
norm_eps = 1e-05
mask_fill = -1e30
log2_e = 1.4426950408889634

LANE = 128
SUB = 8
SLOTS = 6
MAIN = 12
TAIL = 4
MIB = 1 << 20


def call(body, out_shape, vmem_mib, **kwargs):
    return pl.pallas_call(
        body,
        out_shape=out_shape,
        compiler_params=pltpu.CompilerParams(vmem_limit_bytes=vmem_mib * MIB),
        **kwargs,
    )


def dot(a, b, dims=((1,), (0,))):
    return lax.dot_general(a, b, (dims, ((), ())), preferred_element_type=jnp.float32)


def layer_norm(summed, gain_row):
    centre = jnp.mean(summed, axis=-1, keepdims=True)
    centred = summed - centre
    spread = jnp.mean(jnp.square(centred), axis=-1, keepdims=True)
    return centred * lax.rsqrt(spread + norm_eps) * gain_row


def in_hbm(*arrays):
    return tuple(pltpu.with_memory_space_constraint(a, pltpu.HBM) for a in arrays)


def slot_of(place, kind):
    if kind == 0:
        return jnp.where(place < SLOTS, place, -2)
    return jnp.where(place >= SLOTS, place - SLOTS + 2 * (kind - 1), -2)


def prepare_body(
    q_ref,
    k_ref,
    v_ref,
    ids_hbm,
    score_hbm,
    out_ref,
    pick_ref,
    blend_ref,
    ids_ref,
    score_ref,
    land_ref,
    sems,
    small,
):
    lists = [
        pltpu.make_async_copy(ids_hbm, ids_ref, small.at[0]),
        pltpu.make_async_copy(score_hbm, score_ref, small.at[1]),
    ]
    copies = [
        pltpu.make_async_copy(ref.at[0], land_ref.at[n], sems.at[n])
        for n, ref in enumerate((q_ref, k_ref, v_ref))
    ]
    for copy in lists + copies:
        copy.start()
    for copy in lists:
        copy.wait()
    top_k, rows = ids_ref.shape[1:]
    experts = pick_ref.shape[1] // SUB
    expert = lax.broadcasted_iota(jnp.int32, (experts, rows), 0)
    scores = score_ref[0]
    raised = jnp.exp(scores - jnp.max(scores, axis=0, keepdims=True))
    shares = raised / jnp.sum(raised, axis=0, keepdims=True)
    named = jnp.zeros((experts, rows), jnp.float32)
    share = jnp.zeros((experts, rows), jnp.float32)
    for k in range(top_k):
        hit = ids_ref[0, k : k + 1] == expert
        named = jnp.where(hit, 1.0, named)
        share = jnp.where(hit, shares[k : k + 1], share)
    earlier = lax.broadcasted_iota(jnp.int32, (rows, rows), 0) < lax.broadcasted_iota(
        jnp.int32, (rows, rows), 1
    )
    rank = dot(named.astype(jnp.bfloat16), jnp.where(earlier, 1.0, 0.0).astype(jnp.bfloat16))
    slot = jnp.where(named > 0.0, rank, -1.0)
    by_expert = jnp.broadcast_to(slot[:, None, :], (experts, SUB, rows))
    place = lax.broadcasted_iota(jnp.int32, (experts, SUB, rows), 1)
    for kind in range(4):
        hit = by_expert == slot_of(place, kind).astype(jnp.float32)
        pick = jnp.where(hit, 1.0, 0.0).reshape(experts * SUB, rows).astype(jnp.bfloat16)
        pick_ref[kind] = pick
    wide = (experts, experts * SUB)
    spread = lax.broadcasted_iota(jnp.int32, wide, 0) == lax.broadcasted_iota(
        jnp.int32, wide, 1
    ) // SUB
    spread = jnp.where(spread, 1.0, 0.0).astype(jnp.bfloat16)
    wide_slot = dot(slot.T.astype(jnp.bfloat16), spread)
    wide_share = dot(share.T.astype(jnp.bfloat16), spread)
    place = lax.broadcasted_iota(jnp.int32, wide_slot.shape, 1) % SUB
    for kind in range(4):
        hit = wide_slot == slot_of(place, kind).astype(jnp.float32)
        blend_ref[kind] = jnp.where(hit, wide_share, 0.0).astype(jnp.bfloat16)
    for n, copy in enumerate(copies):
        copy.wait()
        for h in range(out_ref.shape[0]):
            out_ref[h, n] = land_ref[n, :, h * LANE : (h + 1) * LANE]


def prepare(q, k, v, ids, scores, experts):
    rows, width = q.shape[1:]
    heads = width // LANE
    near = pl.BlockSpec(memory_space=pltpu.VMEM)
    return call(
        prepare_body,
        (
            pltpu.VMEM((heads, 3, rows, LANE), q.dtype),
            jax.ShapeDtypeStruct((4, experts * SUB, rows), jnp.bfloat16),
            jax.ShapeDtypeStruct((4, rows, experts * SUB), jnp.bfloat16),
        ),
        16,
        in_specs=[pl.BlockSpec(memory_space=pltpu.HBM)] * 5,
        out_specs=(near,) * 3,
        scratch_shapes=[
            pltpu.VMEM(ids.shape, ids.dtype),
            pltpu.VMEM(scores.shape, scores.dtype),
            pltpu.VMEM((3, rows, width), q.dtype),
            pltpu.SemaphoreType.DMA((3,)),
            pltpu.SemaphoreType.DMA((2,)),
        ],
    )(*in_hbm(q, k, v, ids, scores))


def attend_body(qkv_ref, gate_ref, weight_ref, out_ref, near_ref, score_ref, sem):
    brought = pltpu.make_async_copy(weight_ref, near_ref, sem)
    brought.start()
    parts, _, rows, size = qkv_ref.shape
    pair = 2
    block = pair * rows
    scale = size ** (-0.5) * log2_e

    def part(j, n):
        return qkv_ref[pair * j : pair * (j + 1), n].reshape(block, size)

    def score_rows(b):
        q = part(b, 0)
        base = gate_ref[:, block * b : block * b + 1]
        top = jnp.full((block, LANE), mask_fill, jnp.float32)
        for j in range(b + 1):
            bias = (gate_ref[:, block * j : block * (j + 1)] - base) * log2_e
            s = dot(q, part(j, 1), ((1,), (1,))) * scale - bias
            if j == b:
                row = lax.broadcasted_iota(jnp.int32, s.shape, 0)
                col = lax.broadcasted_iota(jnp.int32, s.shape, 1)
                s = jnp.where(row >= col, s, mask_fill)
            score_ref[b % 2, :, block * j : block * (j + 1)] = s
            for c in range(block // LANE):
                top = jnp.maximum(top, s[:, c * LANE : (c + 1) * LANE])
        return jnp.max(top, axis=1, keepdims=True)

    def blend_rows(b, row_max):
        total = jnp.zeros((block, LANE), jnp.float32)
        blended = jnp.zeros((block, size), jnp.float32)
        for j in range(b + 1):
            w = jnp.exp2(score_ref[b % 2, :, block * j : block * (j + 1)] - row_max)
            for c in range(block // LANE):
                total = total + w[:, c * LANE : (c + 1) * LANE]
            blended = blended + dot(w.astype(jnp.bfloat16), part(j, 2))
        row_total = jnp.sum(total, axis=1, keepdims=True)
        done = (blended / row_total).astype(jnp.bfloat16)
        out_ref[pair * b : pair * (b + 1)] = done.reshape(pair, rows, size)

    count = parts // pair
    row_max = score_rows(0)
    for b in range(count):
        ahead = score_rows(b + 1) if b + 1 < count else None
        blend_rows(b, row_max)
        row_max = ahead
    brought.wait()


def attend(qkv, gates, weight):
    parts, _, rows, size = qkv.shape
    near = pl.BlockSpec(memory_space=pltpu.VMEM)
    return call(
        attend_body,
        (
            jax.ShapeDtypeStruct((parts, rows, size), qkv.dtype),
            pltpu.VMEM(weight.shape, weight.dtype),
        ),
        20,
        in_specs=[near, near, pl.BlockSpec(memory_space=pltpu.HBM)],
        out_specs=(near, near),
        scratch_shapes=[
            pltpu.VMEM((2, 2 * rows, parts * rows), jnp.float32),
            pltpu.SemaphoreType.DMA,
        ],
    )(qkv, gates, *in_hbm(weight))


def project_body(heads_ref, stream_ref, weight_ref, gain_ref, pick_ref, first_ref, out_ref):
    heads = heads_ref.shape[0]
    experts = out_ref.shape[0]
    attended = jnp.concatenate([heads_ref[h] for h in range(heads)], axis=1)
    projected = dot(attended, weight_ref[...])
    summed = deep_alpha * stream_ref[0].astype(jnp.float32) + projected
    first = layer_norm(summed, gain_ref[...]).astype(jnp.bfloat16)
    first_ref[...] = first
    tail = first[:, MAIN * LANE :]
    for p in range(3):
        kept = [first[:, (3 * q + p) * LANE : (3 * q + p + 1) * LANE] for q in range(TAIL)]
        both = jnp.concatenate([jnp.concatenate(kept, axis=1), tail], axis=0)
        lhs = jnp.concatenate([pick_ref[0], pick_ref[p + 1]], axis=1)
        rows = dot(lhs, both).astype(jnp.bfloat16)
        for q in range(TAIL):
            tile = rows[:, q * LANE : (q + 1) * LANE]
            out_ref[:, 3 * q + p] = tile.reshape(experts, SUB, LANE)


def project(heads, stream, weight, gain, pick):
    rows, width = stream.shape[1:]
    experts = pick.shape[1] // SUB
    return call(
        project_body,
        (
            jax.ShapeDtypeStruct((rows, width), jnp.bfloat16),
            jax.ShapeDtypeStruct((experts, MAIN, SUB, LANE), jnp.bfloat16),
        ),
        36,
    )(heads, stream, weight, gain, pick)


def expert_body(in_ref, gate_ref, up_ref, down_ref, out_ref):
    sources = in_ref.shape[0]
    rows = sources * SUB
    place = lax.broadcasted_iota(jnp.int32, (rows, LANE), 0) % SUB
    kept = [in_ref[:, t].reshape(rows, LANE) for t in range(MAIN)]
    tail = []
    for q in range(TAIL):
        spare = [
            pltpu.roll(kept[3 * q + p].astype(jnp.float32), rows - SLOTS + 2 * p, 0)
            for p in range(3)
        ]
        block = jnp.where(place < 2, spare[0], jnp.where(place < 4, spare[1], spare[2]))
        tail.append(block.astype(jnp.bfloat16))
    x = jnp.concatenate(kept + tail, axis=1)
    hidden = []
    units = gate_ref.shape[2]
    for lo in range(0, units, units // 2):
        half = slice(lo, lo + units // 2)
        gate_act = jnp.minimum(dot(x, gate_ref[0, :, half]), clamp_limit)
        up_act = jnp.clip(dot(x, up_ref[0, :, half]), -clamp_limit, clamp_limit)
        act = gate_act * jax.nn.sigmoid(swish_alpha * gate_act) * (up_act + 1.0)
        hidden.append(act.astype(jnp.bfloat16))
    hidden = jnp.concatenate(hidden, axis=1)
    y_tail = dot(hidden, down_ref[0, :, MAIN * LANE :])
    for first in range(0, MAIN, TAIL):
        y = dot(hidden, down_ref[0, :, first * LANE : (first + TAIL) * LANE])
        for i in range(TAIL):
            t = first + i
            q, p = t // 3, t % 3
            spare = pltpu.roll(y_tail[:, q * LANE : (q + 1) * LANE], SLOTS - 2 * p, 0)
            tile = jnp.where(place < SLOTS, y[:, i * LANE : (i + 1) * LANE], spare)
            out_ref[:, t] = tile.astype(jnp.bfloat16).reshape(sources, SUB, LANE)


def expert(arrived, gate, up, down):
    sources, step = arrived.shape[0], 64
    block = pl.BlockSpec((step, MAIN, SUB, LANE), lambda i: (i, 0, 0, 0))
    whole = [pl.BlockSpec(w.shape, lambda i: (0, 0, 0)) for w in (gate, up, down)]
    return call(
        expert_body,
        jax.ShapeDtypeStruct(arrived.shape, arrived.dtype),
        36,
        grid=(sources // step,),
        in_specs=[block] + whole,
        out_specs=block,
    )(arrived, gate, up, down)


def combine_body(in_ref, blend_ref, first_ref, gain_ref, out_ref):
    experts = in_ref.shape[0]
    tail = None
    blocks = [None] * MAIN
    for p in range(3):
        rows = [in_ref[:, 3 * q + p].reshape(experts * SUB, LANE) for q in range(TAIL)]
        both = jnp.concatenate([blend_ref[0], blend_ref[p + 1]], axis=0)
        mixed = dot(both, jnp.concatenate(rows, axis=1))
        count = blend_ref.shape[1]
        for q in range(TAIL):
            blocks[3 * q + p] = mixed[:count, q * LANE : (q + 1) * LANE]
        tail = mixed[count:] if tail is None else tail + mixed[count:]
    mixture = jnp.concatenate(blocks + [tail], axis=1)
    summed = deep_alpha * first_ref[...].astype(jnp.float32) + mixture
    out_ref[0] = layer_norm(summed, gain_ref[...]).astype(jnp.bfloat16)


def combine(returned, blend, first, gain):
    return call(
        combine_body,
        jax.ShapeDtypeStruct((1, *first.shape), jnp.bfloat16),
        36,
    )(returned, blend, first, gain)


def exchange(x, axes):
    return lax.all_to_all(x, axes, split_axis=0, concat_axis=0, tiled=True)


def shards(
    stream,
    query_rows,
    key_rows,
    value_rows,
    forget_sums,
    out_weight,
    first_gain,
    expert_ids,
    route_scores,
    gate_weight,
    up_weight,
    down_weight,
    second_gain,
):
    experts = lax.axis_size(SP_DP)
    packed, pick, blend = prepare(
        query_rows,
        key_rows,
        value_rows,
        expert_ids.transpose(0, 2, 1),
        route_scores.transpose(0, 2, 1),
        experts,
    )
    qkv = exchange(packed, SP)
    attended, near_weight = attend(qkv, forget_sums[0], out_weight)
    heads = exchange(attended, SP)
    first, outgoing = project(heads, stream, near_weight, first_gain[None], pick)
    arrived = exchange(outgoing, SP_DP)
    finished = expert(arrived, gate_weight, up_weight, down_weight)
    returned = exchange(finished, SP_DP)
    return combine(returned, blend, first, second_gain[None])


def solution(mesh):
    finer = Mesh(mesh.devices.reshape(4, 4, mesh.shape["dp"]), ("sp_0", "sp_1", "dp"))
    rows = P("dp", SP, None)
    own = P(SP_DP, None, None)
    placed = (rows,) * 5 + (P(), P(), rows, rows, own, own, own, P())
    return jax.shard_map(shards, mesh=finer, in_specs=placed, out_specs=rows, check_vma=False)
```

```python
import jax
import jax.numpy as jnp
from jax import lax
from jax.experimental import pallas as pl
from jax.experimental.pallas import tpu as pltpu
from jax.sharding import Mesh
from jax.sharding import PartitionSpec as P

SP = ("sp_0", "sp_1")
SP_DP = ("sp_0", "sp_1", "dp")

deep_alpha = 8.0**0.25
clamp_limit = 7.0
swish_alpha = 1.702
norm_eps = 1e-05
mask_fill = -1e30
log2_e = 1.4426950408889634

LANE = 128
SUB = 8
SLOTS = 6
MAIN = 12
TAIL = 4
MIB = 1 << 20


def call(body, out_shape, vmem_mib, **kwargs):
    return pl.pallas_call(
        body,
        out_shape=out_shape,
        compiler_params=pltpu.CompilerParams(vmem_limit_bytes=vmem_mib * MIB),
        **kwargs,
    )


def dot(a, b, dims=((1,), (0,))):
    return lax.dot_general(a, b, (dims, ((), ())), preferred_element_type=jnp.float32)


def layer_norm(summed, gain_row):
    centre = jnp.mean(summed, axis=-1, keepdims=True)
    centred = summed - centre
    spread = jnp.mean(jnp.square(centred), axis=-1, keepdims=True)
    return centred * lax.rsqrt(spread + norm_eps) * gain_row


def in_hbm(*arrays):
    return tuple(pltpu.with_memory_space_constraint(a, pltpu.HBM) for a in arrays)


def slot_of(place, kind):
    if kind == 0:
        return jnp.where(place < SLOTS, place, -2)
    return jnp.where(place >= SLOTS, place - SLOTS + 2 * (kind - 1), -2)


def prepare_body(
    q_ref,
    k_ref,
    v_ref,
    ids_hbm,
    score_hbm,
    out_ref,
    pick_ref,
    blend_ref,
    ids_ref,
    score_ref,
    land_ref,
    sems,
    small,
):
    lists = [
        pltpu.make_async_copy(ids_hbm, ids_ref, small.at[0]),
        pltpu.make_async_copy(score_hbm, score_ref, small.at[1]),
    ]
    copies = [
        pltpu.make_async_copy(ref.at[0], land_ref.at[n], sems.at[n])
        for n, ref in enumerate((q_ref, k_ref, v_ref))
    ]
    for copy in lists + copies:
        copy.start()
    for copy in lists:
        copy.wait()
    top_k, rows = ids_ref.shape[1:]
    experts = pick_ref.shape[1] // SUB
    expert = lax.broadcasted_iota(jnp.int32, (experts, rows), 0)
    scores = score_ref[0]
    raised = jnp.exp(scores - jnp.max(scores, axis=0, keepdims=True))
    shares = raised / jnp.sum(raised, axis=0, keepdims=True)
    named = jnp.zeros((experts, rows), jnp.float32)
    share = jnp.zeros((experts, rows), jnp.float32)
    for k in range(top_k):
        hit = ids_ref[0, k : k + 1] == expert
        named = jnp.where(hit, 1.0, named)
        share = jnp.where(hit, shares[k : k + 1], share)
    earlier = lax.broadcasted_iota(jnp.int32, (rows, rows), 0) < lax.broadcasted_iota(
        jnp.int32, (rows, rows), 1
    )
    rank = dot(named.astype(jnp.bfloat16), jnp.where(earlier, 1.0, 0.0).astype(jnp.bfloat16))
    slot = jnp.where(named > 0.0, rank, -1.0)
    by_expert = jnp.broadcast_to(slot[:, None, :], (experts, SUB, rows))
    place = lax.broadcasted_iota(jnp.int32, (experts, SUB, rows), 1)
    for kind in range(4):
        hit = by_expert == slot_of(place, kind).astype(jnp.float32)
        pick = jnp.where(hit, 1.0, 0.0).reshape(experts * SUB, rows).astype(jnp.bfloat16)
        pick_ref[kind] = pick
    wide = (experts, experts * SUB)
    spread = lax.broadcasted_iota(jnp.int32, wide, 0) == lax.broadcasted_iota(
        jnp.int32, wide, 1
    ) // SUB
    spread = jnp.where(spread, 1.0, 0.0).astype(jnp.bfloat16)
    wide_slot = dot(slot.T.astype(jnp.bfloat16), spread)
    wide_share = dot(share.T.astype(jnp.bfloat16), spread)
    place = lax.broadcasted_iota(jnp.int32, wide_slot.shape, 1) % SUB
    for kind in range(4):
        hit = wide_slot == slot_of(place, kind).astype(jnp.float32)
        blend_ref[kind] = jnp.where(hit, wide_share, 0.0).astype(jnp.bfloat16)
    for n, copy in enumerate(copies):
        copy.wait()
        for h in range(out_ref.shape[0]):
            out_ref[h, n] = land_ref[n, :, h * LANE : (h + 1) * LANE]


def prepare(q, k, v, ids, scores, experts):
    rows, width = q.shape[1:]
    heads = width // LANE
    near = pl.BlockSpec(memory_space=pltpu.VMEM)
    return call(
        prepare_body,
        (
            pltpu.VMEM((heads, 3, rows, LANE), q.dtype),
            jax.ShapeDtypeStruct((4, experts * SUB, rows), jnp.bfloat16),
            jax.ShapeDtypeStruct((4, rows, experts * SUB), jnp.bfloat16),
        ),
        16,
        in_specs=[pl.BlockSpec(memory_space=pltpu.HBM)] * 5,
        out_specs=(near,) * 3,
        scratch_shapes=[
            pltpu.VMEM(ids.shape, ids.dtype),
            pltpu.VMEM(scores.shape, scores.dtype),
            pltpu.VMEM((3, rows, width), q.dtype),
            pltpu.SemaphoreType.DMA((3,)),
            pltpu.SemaphoreType.DMA((2,)),
        ],
    )(*in_hbm(q, k, v, ids, scores))


def attend_body(qkv_ref, gate_ref, weight_ref, out_ref, near_ref, score_ref, sem):
    brought = pltpu.make_async_copy(weight_ref, near_ref, sem)
    brought.start()
    parts, _, rows, size = qkv_ref.shape
    pair = 2
    block = pair * rows
    scale = size ** (-0.5) * log2_e

    def part(j, n):
        return qkv_ref[pair * j : pair * (j + 1), n].reshape(block, size)

    def score_rows(b):
        q = part(b, 0)
        base = gate_ref[:, block * b : block * b + 1]
        top = jnp.full((block, LANE), mask_fill, jnp.float32)
        for j in range(b + 1):
            bias = (gate_ref[:, block * j : block * (j + 1)] - base) * log2_e
            s = dot(q, part(j, 1), ((1,), (1,))) * scale - bias
            if j == b:
                row = lax.broadcasted_iota(jnp.int32, s.shape, 0)
                col = lax.broadcasted_iota(jnp.int32, s.shape, 1)
                s = jnp.where(row >= col, s, mask_fill)
            score_ref[b % 2, :, block * j : block * (j + 1)] = s
            for c in range(block // LANE):
                top = jnp.maximum(top, s[:, c * LANE : (c + 1) * LANE])
        return jnp.max(top, axis=1, keepdims=True)

    def blend_rows(b, row_max):
        total = jnp.zeros((block, LANE), jnp.float32)
        blended = jnp.zeros((block, size), jnp.float32)
        for j in range(b + 1):
            w = jnp.exp2(score_ref[b % 2, :, block * j : block * (j + 1)] - row_max)
            for c in range(block // LANE):
                total = total + w[:, c * LANE : (c + 1) * LANE]
            blended = blended + dot(w.astype(jnp.bfloat16), part(j, 2))
        row_total = jnp.sum(total, axis=1, keepdims=True)
        done = (blended / row_total).astype(jnp.bfloat16)
        out_ref[pair * b : pair * (b + 1)] = done.reshape(pair, rows, size)

    last = parts // pair - 1
    row_max = score_rows(last)
    for b in range(last, -1, -1):
        ahead = score_rows(b - 1) if b > 0 else None
        blend_rows(b, row_max)
        row_max = ahead
    brought.wait()


def attend(qkv, gates, weight):
    parts, _, rows, size = qkv.shape
    near = pl.BlockSpec(memory_space=pltpu.VMEM)
    return call(
        attend_body,
        (
            jax.ShapeDtypeStruct((parts, rows, size), qkv.dtype),
            pltpu.VMEM(weight.shape, weight.dtype),
        ),
        20,
        in_specs=[near, near, pl.BlockSpec(memory_space=pltpu.HBM)],
        out_specs=(near, near),
        scratch_shapes=[
            pltpu.VMEM((2, 2 * rows, parts * rows), jnp.float32),
            pltpu.SemaphoreType.DMA,
        ],
    )(qkv, gates, *in_hbm(weight))


def project_body(heads_ref, stream_ref, weight_ref, gain_ref, pick_ref, first_ref, out_ref):
    heads = heads_ref.shape[0]
    experts = out_ref.shape[0]
    attended = jnp.concatenate([heads_ref[h] for h in range(heads)], axis=1)
    projected = dot(attended, weight_ref[...])
    summed = deep_alpha * stream_ref[0].astype(jnp.float32) + projected
    first = layer_norm(summed, gain_ref[...]).astype(jnp.bfloat16)
    first_ref[...] = first
    tail = first[:, MAIN * LANE :]
    for p in range(3):
        kept = [first[:, (3 * q + p) * LANE : (3 * q + p + 1) * LANE] for q in range(TAIL)]
        both = jnp.concatenate([jnp.concatenate(kept, axis=1), tail], axis=0)
        lhs = jnp.concatenate([pick_ref[0], pick_ref[p + 1]], axis=1)
        rows = dot(lhs, both).astype(jnp.bfloat16)
        for q in range(TAIL):
            tile = rows[:, q * LANE : (q + 1) * LANE]
            out_ref[:, 3 * q + p] = tile.reshape(experts, SUB, LANE)


def project(heads, stream, weight, gain, pick):
    rows, width = stream.shape[1:]
    experts = pick.shape[1] // SUB
    return call(
        project_body,
        (
            jax.ShapeDtypeStruct((rows, width), jnp.bfloat16),
            jax.ShapeDtypeStruct((experts, MAIN, SUB, LANE), jnp.bfloat16),
        ),
        36,
    )(heads, stream, weight, gain, pick)


def expert_body(in_ref, gate_ref, up_ref, down_ref, out_ref):
    groups = in_ref.shape[0]
    rows = groups * SUB
    place = lax.broadcasted_iota(jnp.int32, (rows, LANE), 0) % SUB
    units = gate_ref.shape[2]

    def moved(x, places):
        return pltpu.roll(x, places % rows, 0)

    def by_place(first, second, third, spare):
        rest = jnp.where(place < 4, second, jnp.where(place < SLOTS, third, spare))
        return jnp.where(place < 2, first, rest)

    came = [
        [in_ref[:, i, t].reshape(rows, LANE).astype(jnp.float32) for t in range(MAIN)]
        for i in range(4)
    ]
    x = []
    for i in range(3):
        blocks = [
            jnp.where(place < SLOTS, came[i][t], moved(came[3][t], SLOTS - 2 * i))
            for t in range(MAIN)
        ]
        for q in range(TAIL):
            own = [moved(came[i][3 * q + p], 2 * p - SLOTS) for p in range(3)]
            blocks.append(by_place(*own, came[3][3 * q + i]))
        x.append(jnp.concatenate([block.astype(jnp.bfloat16) for block in blocks], axis=1))
    x = jnp.concatenate(x, axis=0)
    hidden = []
    for lo in range(0, units, units // 2):
        half = slice(lo, lo + units // 2)
        gate_act = jnp.minimum(dot(x, gate_ref[0, :, half]), clamp_limit)
        up_act = jnp.clip(dot(x, up_ref[0, :, half]), -clamp_limit, clamp_limit)
        act = gate_act * jax.nn.sigmoid(swish_alpha * gate_act) * (up_act + 1.0)
        hidden.append(act.astype(jnp.bfloat16))
    hidden = jnp.concatenate(hidden, axis=1)
    y_tail = dot(hidden, down_ref[0, :, MAIN * LANE :])

    def part(y, i, c):
        return y[i * rows : (i + 1) * rows, c * LANE : (c + 1) * LANE]

    for first in range(0, MAIN, TAIL):
        y = dot(hidden, down_ref[0, :, first * LANE : (first + TAIL) * LANE])
        for c in range(TAIL):
            t = first + c
            q, p = t // 3, t % 3
            tiles = [
                jnp.where(place < SLOTS, part(y, i, c), moved(part(y_tail, i, q), SLOTS - 2 * p))
                for i in range(3)
            ]
            lent = [moved(part(y, i, c), 2 * i - SLOTS) for i in range(3)]
            tiles.append(by_place(*lent, part(y_tail, p, q)))
            for i, tile in enumerate(tiles):
                out_ref[:, i, t] = tile.astype(jnp.bfloat16).reshape(groups, SUB, LANE)


def expert(arrived, gate, up, down):
    sources, step = arrived.shape[0], 32
    fours = arrived.reshape(sources // 4, 4, *arrived.shape[1:])
    block = pl.BlockSpec((step // 4, *fours.shape[1:]), lambda i: (i, 0, 0, 0, 0))
    whole = [pl.BlockSpec(w.shape, lambda i: (0, 0, 0)) for w in (gate, up, down)]
    return call(
        expert_body,
        jax.ShapeDtypeStruct(fours.shape, fours.dtype),
        30,
        grid=(sources // step,),
        in_specs=[block] + whole,
        out_specs=block,
    )(fours, gate, up, down).reshape(arrived.shape)


def combine_body(in_ref, blend_ref, first_ref, gain_ref, out_ref):
    experts = in_ref.shape[0]
    tail = None
    blocks = [None] * MAIN
    for p in range(3):
        rows = [in_ref[:, 3 * q + p].reshape(experts * SUB, LANE) for q in range(TAIL)]
        both = jnp.concatenate([blend_ref[0], blend_ref[p + 1]], axis=0)
        mixed = dot(both, jnp.concatenate(rows, axis=1))
        count = blend_ref.shape[1]
        for q in range(TAIL):
            blocks[3 * q + p] = mixed[:count, q * LANE : (q + 1) * LANE]
        tail = mixed[count:] if tail is None else tail + mixed[count:]
    mixture = jnp.concatenate(blocks + [tail], axis=1)
    summed = deep_alpha * first_ref[...].astype(jnp.float32) + mixture
    out_ref[0] = layer_norm(summed, gain_ref[...]).astype(jnp.bfloat16)


def combine(returned, blend, first, gain):
    return call(
        combine_body,
        jax.ShapeDtypeStruct((1, *first.shape), jnp.bfloat16),
        36,
    )(returned, blend, first, gain)


def exchange(x, axes):
    return lax.all_to_all(x, axes, split_axis=0, concat_axis=0, tiled=True)


def shards(
    stream,
    query_rows,
    key_rows,
    value_rows,
    forget_sums,
    out_weight,
    first_gain,
    expert_ids,
    route_scores,
    gate_weight,
    up_weight,
    down_weight,
    second_gain,
):
    experts = lax.axis_size(SP_DP)
    packed, pick, blend = prepare(
        query_rows,
        key_rows,
        value_rows,
        expert_ids.transpose(0, 2, 1),
        route_scores.transpose(0, 2, 1),
        experts,
    )
    qkv = exchange(packed, SP)
    attended, near_weight = attend(qkv, forget_sums[0], out_weight)
    heads = exchange(attended, SP)
    first, outgoing = project(heads, stream, near_weight, first_gain[None], pick)
    arrived = exchange(outgoing, SP_DP)
    finished = expert(arrived, gate_weight, up_weight, down_weight)
    returned = exchange(finished, SP_DP)
    return combine(returned, blend, first, second_gain[None])


def solution(mesh):
    finer = Mesh(mesh.devices.reshape(4, 4, mesh.shape["dp"]), ("sp_0", "sp_1", "dp"))
    rows = P("dp", SP, None)
    own = P(SP_DP, None, None)
    placed = (rows,) * 5 + (P(), P(), rows, rows, own, own, own, P())
    return jax.shard_map(shards, mesh=finer, in_specs=placed, out_specs=rows, check_vma=False)
```

```python
import jax
import jax.numpy as jnp
from jax import lax
from jax.experimental import pallas as pl
from jax.experimental.pallas import tpu as pltpu
from jax.sharding import Mesh
from jax.sharding import PartitionSpec as P

SP = ("sp_0", "sp_1")
SP_DP = ("sp_0", "sp_1", "dp")

deep_alpha = 8.0**0.25
clamp_limit = 7.0
swish_alpha = 1.702
norm_eps = 1e-05
mask_fill = -1e30
log2_e = 1.4426950408889634

LANE = 128
SUB = 8
SLOTS = 6
MAIN = 12
TAIL = 4
MIB = 1 << 20


def call(body, out_shape, vmem_mib, **kwargs):
    return pl.pallas_call(
        body,
        out_shape=out_shape,
        compiler_params=pltpu.CompilerParams(vmem_limit_bytes=vmem_mib * MIB),
        **kwargs,
    )


def dot(a, b, dims=((1,), (0,))):
    return lax.dot_general(a, b, (dims, ((), ())), preferred_element_type=jnp.float32)


def layer_norm(summed, gain_row):
    centre = jnp.mean(summed, axis=-1, keepdims=True)
    centred = summed - centre
    spread = jnp.mean(jnp.square(centred), axis=-1, keepdims=True)
    return centred * lax.rsqrt(spread + norm_eps) * gain_row


def in_hbm(*arrays):
    return tuple(pltpu.with_memory_space_constraint(a, pltpu.HBM) for a in arrays)


def pack_body(q_ref, k_ref, v_ref, out_ref, land_ref, sems):
    copies = [
        pltpu.make_async_copy(ref.at[0], land_ref.at[n], sems.at[n])
        for n, ref in enumerate((q_ref, k_ref, v_ref))
    ]
    for copy in copies:
        copy.start()
    for n, copy in enumerate(copies):
        copy.wait()
        for h in range(out_ref.shape[0]):
            out_ref[h, n] = land_ref[n, :, h * LANE : (h + 1) * LANE]


def pack(q, k, v):
    rows, width = q.shape[1:]
    return call(
        pack_body,
        pltpu.VMEM((width // LANE, 3, rows, LANE), q.dtype),
        8,
        in_specs=[pl.BlockSpec(memory_space=pltpu.HBM)] * 3,
        out_specs=pl.BlockSpec(memory_space=pltpu.VMEM),
        scratch_shapes=[
            pltpu.VMEM((3, rows, width), q.dtype),
            pltpu.SemaphoreType.DMA((3,)),
        ],
    )(*in_hbm(q, k, v))


def attend_body(qkv_ref, gate_ref, weight_ref, out_ref, near_ref, score_ref, sem):
    brought = pltpu.make_async_copy(weight_ref, near_ref, sem)
    brought.start()
    parts, _, rows, size = qkv_ref.shape
    pair = 2
    block = pair * rows
    scale = size ** (-0.5) * log2_e

    def part(j, n):
        return qkv_ref[pair * j : pair * (j + 1), n].reshape(block, size)

    def score_rows(b):
        q = part(b, 0)
        base = gate_ref[:, block * b : block * b + 1]
        top = jnp.full((block, LANE), mask_fill, jnp.float32)
        for j in range(b + 1):
            bias = (gate_ref[:, block * j : block * (j + 1)] - base) * log2_e
            s = dot(q, part(j, 1), ((1,), (1,))) * scale - bias
            if j == b:
                row = lax.broadcasted_iota(jnp.int32, s.shape, 0)
                col = lax.broadcasted_iota(jnp.int32, s.shape, 1)
                s = jnp.where(row >= col, s, mask_fill)
            score_ref[b % 2, :, block * j : block * (j + 1)] = s
            for c in range(block // LANE):
                top = jnp.maximum(top, s[:, c * LANE : (c + 1) * LANE])
        return jnp.max(top, axis=1, keepdims=True)

    def blend_rows(b, row_max):
        total = jnp.zeros((block, LANE), jnp.float32)
        blended = jnp.zeros((block, size), jnp.float32)
        for j in range(b + 1):
            w = jnp.exp2(score_ref[b % 2, :, block * j : block * (j + 1)] - row_max)
            for c in range(block // LANE):
                total = total + w[:, c * LANE : (c + 1) * LANE]
            blended = blended + dot(w.astype(jnp.bfloat16), part(j, 2))
        row_total = jnp.sum(total, axis=1, keepdims=True)
        done = (blended / row_total).astype(jnp.bfloat16)
        out_ref[pair * b : pair * (b + 1)] = done.reshape(pair, rows, size)

    last = parts // pair - 1
    row_max = score_rows(last)
    for b in range(last, -1, -1):
        ahead = score_rows(b - 1) if b > 0 else None
        blend_rows(b, row_max)
        row_max = ahead
    brought.wait()


def attend(qkv, gates, weight):
    parts, _, rows, size = qkv.shape
    near = pl.BlockSpec(memory_space=pltpu.VMEM)
    return call(
        attend_body,
        (
            jax.ShapeDtypeStruct((parts, rows, size), qkv.dtype),
            pltpu.VMEM(weight.shape, weight.dtype),
        ),
        20,
        in_specs=[near, near, pl.BlockSpec(memory_space=pltpu.HBM)],
        out_specs=(near, near),
        scratch_shapes=[
            pltpu.VMEM((2, 2 * rows, parts * rows), jnp.float32),
            pltpu.SemaphoreType.DMA,
        ],
    )(qkv, gates, *in_hbm(weight))


def slot_of(place, kind):
    if kind == 0:
        return jnp.where(place < SLOTS, place, -2)
    return jnp.where(place >= SLOTS, place - SLOTS + 2 * (kind - 1), -2)


def route_into(ids_ref, score_ref, pick_ref, blend_ref):
    top_k, rows = ids_ref.shape[1:]
    experts = pick_ref.shape[1] // SUB
    expert = lax.broadcasted_iota(jnp.int32, (experts, rows), 0)
    scores = score_ref[0]
    raised = jnp.exp(scores - jnp.max(scores, axis=0, keepdims=True))
    shares = raised / jnp.sum(raised, axis=0, keepdims=True)
    named = jnp.zeros((experts, rows), jnp.float32)
    share = jnp.zeros((experts, rows), jnp.float32)
    for k in range(top_k):
        hit = ids_ref[0, k : k + 1] == expert
        named = jnp.where(hit, 1.0, named)
        share = jnp.where(hit, shares[k : k + 1], share)
    earlier = lax.broadcasted_iota(jnp.int32, (rows, rows), 0) < lax.broadcasted_iota(
        jnp.int32, (rows, rows), 1
    )
    rank = dot(named.astype(jnp.bfloat16), jnp.where(earlier, 1.0, 0.0).astype(jnp.bfloat16))
    slot = jnp.where(named > 0.0, rank, -1.0)
    by_expert = jnp.broadcast_to(slot[:, None, :], (experts, SUB, rows))
    place = lax.broadcasted_iota(jnp.int32, (experts, SUB, rows), 1)
    for kind in range(4):
        hit = by_expert == slot_of(place, kind).astype(jnp.float32)
        pick = jnp.where(hit, 1.0, 0.0).reshape(experts * SUB, rows).astype(jnp.bfloat16)
        pick_ref[kind] = pick
    wide = (experts, experts * SUB)
    spread = lax.broadcasted_iota(jnp.int32, wide, 0) == lax.broadcasted_iota(
        jnp.int32, wide, 1
    ) // SUB
    spread = jnp.where(spread, 1.0, 0.0).astype(jnp.bfloat16)
    wide_slot = dot(slot.T.astype(jnp.bfloat16), spread)
    wide_share = dot(share.T.astype(jnp.bfloat16), spread)
    place = lax.broadcasted_iota(jnp.int32, wide_slot.shape, 1) % SUB
    for kind in range(4):
        hit = wide_slot == slot_of(place, kind).astype(jnp.float32)
        blend_ref[kind] = jnp.where(hit, wide_share, 0.0).astype(jnp.bfloat16)


def project_body(
    heads_ref,
    stream_ref,
    weight_ref,
    gain_ref,
    ids_ref,
    score_ref,
    first_ref,
    out_ref,
    blend_ref,
    pick_ref,
):
    heads = heads_ref.shape[0]
    experts = out_ref.shape[0]
    attended = jnp.concatenate([heads_ref[h] for h in range(heads)], axis=1)
    projected = dot(attended, weight_ref[...])
    route_into(ids_ref, score_ref, pick_ref, blend_ref)
    summed = deep_alpha * stream_ref[0].astype(jnp.float32) + projected
    first = layer_norm(summed, gain_ref[...]).astype(jnp.bfloat16)
    first_ref[...] = first
    tail = first[:, MAIN * LANE :]
    for p in range(3):
        kept = [first[:, (3 * q + p) * LANE : (3 * q + p + 1) * LANE] for q in range(TAIL)]
        both = jnp.concatenate([jnp.concatenate(kept, axis=1), tail], axis=0)
        lhs = jnp.concatenate([pick_ref[0], pick_ref[p + 1]], axis=1)
        rows = dot(lhs, both).astype(jnp.bfloat16)
        for q in range(TAIL):
            tile = rows[:, q * LANE : (q + 1) * LANE]
            out_ref[:, 3 * q + p] = tile.reshape(experts, SUB, LANE)


def project(heads, stream, weight, gain, ids, scores, experts):
    rows, width = stream.shape[1:]
    return call(
        project_body,
        (
            jax.ShapeDtypeStruct((rows, width), jnp.bfloat16),
            jax.ShapeDtypeStruct((experts, MAIN, SUB, LANE), jnp.bfloat16),
            jax.ShapeDtypeStruct((4, rows, experts * SUB), jnp.bfloat16),
        ),
        36,
        scratch_shapes=[pltpu.VMEM((4, experts * SUB, rows), jnp.bfloat16)],
    )(heads, stream, weight, gain, ids, scores)


def expert_body(in_ref, gate_ref, up_ref, down_ref, out_ref):
    groups = in_ref.shape[0]
    rows = groups * SUB
    units = gate_ref.shape[2]
    place = lax.broadcasted_iota(jnp.int32, (rows, LANE), 0) % SUB
    place = place.astype(jnp.int16)
    below = [place < jnp.int16(n) for n in (2, 4, SLOTS)]

    def moved(x, places):
        return pltpu.roll(x, places % rows, 0)

    def by_place(first, second, third, spare):
        rest = jnp.where(below[1], second, jnp.where(below[2], third, spare))
        return jnp.where(below[0], first, rest)

    came = [[in_ref[:, i, t].reshape(rows, LANE) for t in range(MAIN)] for i in range(4)]
    x = []
    for i in range(3):
        blocks = [
            jnp.where(below[2], came[i][t], moved(came[3][t], SLOTS - 2 * i)) for t in range(MAIN)
        ]
        for q in range(TAIL):
            own = [moved(came[i][3 * q + p], 2 * p - SLOTS) for p in range(3)]
            blocks.append(by_place(*own, came[3][3 * q + i]))
        x.append(jnp.concatenate(blocks, axis=1))
    x = jnp.concatenate(x, axis=0)
    hidden = []
    for lo in range(0, units, units // 2):
        half = slice(lo, lo + units // 2)
        gate_act = jnp.minimum(dot(x, gate_ref[0, :, half]), clamp_limit)
        up_act = jnp.clip(dot(x, up_ref[0, :, half]), -clamp_limit, clamp_limit)
        act = gate_act * jax.nn.sigmoid(swish_alpha * gate_act) * (up_act + 1.0)
        hidden.append(act.astype(jnp.bfloat16))
    hidden = jnp.concatenate(hidden, axis=1)
    y_tail = dot(hidden, down_ref[0, :, MAIN * LANE :]).astype(jnp.bfloat16)

    def part(y, i, c):
        return y[i * rows : (i + 1) * rows, c * LANE : (c + 1) * LANE]

    for first in range(0, MAIN, TAIL):
        y = dot(hidden, down_ref[0, :, first * LANE : (first + TAIL) * LANE])
        y = y.astype(jnp.bfloat16)
        for c in range(TAIL):
            t = first + c
            q, p = t // 3, t % 3
            tiles = [
                jnp.where(below[2], part(y, i, c), moved(part(y_tail, i, q), SLOTS - 2 * p))
                for i in range(3)
            ]
            lent = [moved(part(y, i, c), 2 * i - SLOTS) for i in range(3)]
            tiles.append(by_place(*lent, part(y_tail, p, q)))
            for i, tile in enumerate(tiles):
                out_ref[:, i, t] = tile.reshape(groups, SUB, LANE)


def expert(arrived, gate, up, down):
    sources, step = arrived.shape[0], 64
    fours = arrived.reshape(sources // 4, 4, *arrived.shape[1:])
    block = pl.BlockSpec((step // 4, *fours.shape[1:]), lambda i: (i, 0, 0, 0, 0))
    whole = [pl.BlockSpec(w.shape, lambda i: (0, 0, 0)) for w in (gate, up, down)]
    return call(
        expert_body,
        jax.ShapeDtypeStruct(fours.shape, fours.dtype),
        30,
        grid=(sources // step,),
        in_specs=[block] + whole,
        out_specs=block,
    )(fours, gate, up, down).reshape(arrived.shape)


def combine_body(in_ref, blend_ref, first_ref, gain_ref, out_ref):
    experts = in_ref.shape[0]
    tail = None
    blocks = [None] * MAIN
    for p in range(3):
        rows = [in_ref[:, 3 * q + p].reshape(experts * SUB, LANE) for q in range(TAIL)]
        both = jnp.concatenate([blend_ref[0], blend_ref[p + 1]], axis=0)
        mixed = dot(both, jnp.concatenate(rows, axis=1))
        count = blend_ref.shape[1]
        for q in range(TAIL):
            blocks[3 * q + p] = mixed[:count, q * LANE : (q + 1) * LANE]
        tail = mixed[count:] if tail is None else tail + mixed[count:]
    mixture = jnp.concatenate(blocks + [tail], axis=1)
    summed = deep_alpha * first_ref[...].astype(jnp.float32) + mixture
    out_ref[0] = layer_norm(summed, gain_ref[...]).astype(jnp.bfloat16)


def combine(returned, blend, first, gain):
    return call(
        combine_body,
        jax.ShapeDtypeStruct((1, *first.shape), jnp.bfloat16),
        36,
    )(returned, blend, first, gain)


def exchange(x, axes):
    return lax.all_to_all(x, axes, split_axis=0, concat_axis=0, tiled=True)


def shards(
    stream,
    query_rows,
    key_rows,
    value_rows,
    forget_sums,
    out_weight,
    first_gain,
    expert_ids,
    route_scores,
    gate_weight,
    up_weight,
    down_weight,
    second_gain,
):
    experts = lax.axis_size(SP_DP)
    qkv = exchange(pack(query_rows, key_rows, value_rows), SP)
    attended, near_weight = attend(qkv, forget_sums[0], out_weight)
    heads = exchange(attended, SP)
    first, outgoing, blend = project(
        heads,
        stream,
        near_weight,
        first_gain[None],
        expert_ids.transpose(0, 2, 1),
        route_scores.transpose(0, 2, 1),
        experts,
    )
    arrived = exchange(outgoing, SP_DP)
    finished = expert(arrived, gate_weight, up_weight, down_weight)
    returned = exchange(finished, SP_DP)
    return combine(returned, blend, first, second_gain[None])


def solution(mesh):
    finer = Mesh(mesh.devices.reshape(4, 4, mesh.shape["dp"]), ("sp_0", "sp_1", "dp"))
    rows = P("dp", SP, None)
    own = P(SP_DP, None, None)
    placed = (rows,) * 5 + (P(), P(), rows, rows, own, own, own, P())
    return jax.shard_map(shards, mesh=finer, in_specs=placed, out_specs=rows, check_vma=False)
```

```python
import functools

import jax
import jax.numpy as jnp
from jax import lax
from jax.experimental import pallas as pl
from jax.experimental.pallas import tpu as pltpu
from jax.sharding import Mesh
from jax.sharding import PartitionSpec as P

SP = ("sp_0", "sp_1")
SP_DP = ("sp_0", "sp_1", "dp")
DP_SP = ("dp", "sp_0", "sp_1")

deep_alpha = 8.0**0.25
clamp_limit = 7.0
swish_alpha = 1.702
norm_eps = 1e-05
mask_fill = -1e30
log2_e = 1.4426950408889634

LANE = 128
SUB = 8
SLOTS = 6
MAIN = 12
TAIL = 4
MIB = 1 << 20


def call(body, out_shape, vmem_mib, **kwargs):
    return pl.pallas_call(
        body,
        out_shape=out_shape,
        compiler_params=pltpu.CompilerParams(vmem_limit_bytes=vmem_mib * MIB),
        **kwargs,
    )


def dot(a, b, dims=((1,), (0,))):
    return lax.dot_general(a, b, (dims, ((), ())), preferred_element_type=jnp.float32)


def layer_norm(summed, gain_row):
    centre = jnp.mean(summed, axis=-1, keepdims=True)
    centred = summed - centre
    spread = jnp.mean(jnp.square(centred), axis=-1, keepdims=True)
    return centred * lax.rsqrt(spread + norm_eps) * gain_row


def in_hbm(*arrays):
    return tuple(pltpu.with_memory_space_constraint(a, pltpu.HBM) for a in arrays)


def pack_body(q_ref, k_ref, v_ref, out_ref, land_ref, sems):
    copies = [
        pltpu.make_async_copy(ref.at[0], land_ref.at[n], sems.at[n])
        for n, ref in enumerate((q_ref, k_ref, v_ref))
    ]
    for copy in copies:
        copy.start()
    for n, copy in enumerate(copies):
        copy.wait()
        for h in range(out_ref.shape[0]):
            out_ref[h, n] = land_ref[n, :, h * LANE : (h + 1) * LANE]


def pack(q, k, v):
    rows, width = q.shape[1:]
    return call(
        pack_body,
        pltpu.VMEM((width // LANE, 3, rows, LANE), q.dtype),
        8,
        in_specs=[pl.BlockSpec(memory_space=pltpu.HBM)] * 3,
        out_specs=pl.BlockSpec(memory_space=pltpu.VMEM),
        scratch_shapes=[
            pltpu.VMEM((3, rows, width), q.dtype),
            pltpu.SemaphoreType.DMA((3,)),
        ],
    )(*in_hbm(q, k, v))


def attend_body(qkv_ref, gate_ref, weight_ref, out_ref, near_ref, score_ref, sem):
    brought = pltpu.make_async_copy(weight_ref, near_ref, sem)
    brought.start()
    parts, _, rows, size = qkv_ref.shape
    pair = 2
    block = pair * rows
    scale = size ** (-0.5) * log2_e

    def part(j, n):
        return qkv_ref[pair * j : pair * (j + 1), n].reshape(block, size)

    def score_rows(b):
        q = part(b, 0)
        base = gate_ref[:, block * b : block * b + 1]
        top = jnp.full((block, LANE), mask_fill, jnp.float32)
        for j in range(b + 1):
            bias = (gate_ref[:, block * j : block * (j + 1)] - base) * log2_e
            s = dot(q, part(j, 1), ((1,), (1,))) * scale - bias
            if j == b:
                row = lax.broadcasted_iota(jnp.int32, s.shape, 0)
                col = lax.broadcasted_iota(jnp.int32, s.shape, 1)
                s = jnp.where(row >= col, s, mask_fill)
            score_ref[b % 2, :, block * j : block * (j + 1)] = s
            for c in range(block // LANE):
                top = jnp.maximum(top, s[:, c * LANE : (c + 1) * LANE])
        return jnp.max(top, axis=1, keepdims=True)

    def blend_rows(b, row_max):
        total = jnp.zeros((block, LANE), jnp.float32)
        blended = jnp.zeros((block, size), jnp.float32)
        for j in range(b + 1):
            w = jnp.exp2(score_ref[b % 2, :, block * j : block * (j + 1)] - row_max)
            for c in range(block // LANE):
                total = total + w[:, c * LANE : (c + 1) * LANE]
            blended = blended + dot(w.astype(jnp.bfloat16), part(j, 2))
        row_total = jnp.sum(total, axis=1, keepdims=True)
        done = (blended / row_total).astype(jnp.bfloat16)
        out_ref[pair * b : pair * (b + 1)] = done.reshape(pair, rows, size)

    last = parts // pair - 1
    row_max = score_rows(last)
    for b in range(last, -1, -1):
        ahead = score_rows(b - 1) if b > 0 else None
        blend_rows(b, row_max)
        row_max = ahead
    brought.wait()


def attend(qkv, gates, weight):
    parts, _, rows, size = qkv.shape
    near = pl.BlockSpec(memory_space=pltpu.VMEM)
    return call(
        attend_body,
        (
            jax.ShapeDtypeStruct((parts, rows, size), qkv.dtype),
            pltpu.VMEM(weight.shape, weight.dtype),
        ),
        20,
        in_specs=[near, near, pl.BlockSpec(memory_space=pltpu.HBM)],
        out_specs=(near, near),
        scratch_shapes=[
            pltpu.VMEM((2, 2 * rows, parts * rows), jnp.float32),
            pltpu.SemaphoreType.DMA,
        ],
    )(qkv, gates, *in_hbm(weight))


def slot_of(place, kind):
    if kind == 0:
        return jnp.where(place < SLOTS, place, -2)
    return jnp.where(place >= SLOTS, place - SLOTS + 2 * (kind - 1), -2)


def route_into(ids_ref, score_ref, pick_ref, blend_ref, dp_count):
    top_k, rows = ids_ref.shape[1:]
    experts = pick_ref.shape[1] // SUB
    turn = lax.broadcasted_iota(jnp.int32, (experts, rows), 0)
    sp_count = experts // dp_count
    expert = turn % sp_count * dp_count + turn // sp_count
    scores = score_ref[0]
    raised = jnp.exp(scores - jnp.max(scores, axis=0, keepdims=True))
    shares = raised / jnp.sum(raised, axis=0, keepdims=True)
    named = jnp.zeros((experts, rows), jnp.float32)
    share = jnp.zeros((experts, rows), jnp.float32)
    for k in range(top_k):
        hit = ids_ref[0, k : k + 1] == expert
        named = jnp.where(hit, 1.0, named)
        share = jnp.where(hit, shares[k : k + 1], share)
    earlier = lax.broadcasted_iota(jnp.int32, (rows, rows), 0) < lax.broadcasted_iota(
        jnp.int32, (rows, rows), 1
    )
    rank = dot(named.astype(jnp.bfloat16), jnp.where(earlier, 1.0, 0.0).astype(jnp.bfloat16))
    slot = jnp.where(named > 0.0, rank, -1.0)
    by_expert = jnp.broadcast_to(slot[:, None, :], (experts, SUB, rows))
    place = lax.broadcasted_iota(jnp.int32, (experts, SUB, rows), 1)
    for kind in range(4):
        hit = by_expert == slot_of(place, kind).astype(jnp.float32)
        pick = jnp.where(hit, 1.0, 0.0).reshape(experts * SUB, rows).astype(jnp.bfloat16)
        pick_ref[kind] = pick
    wide = (experts, experts * SUB)
    spread = lax.broadcasted_iota(jnp.int32, wide, 0) == lax.broadcasted_iota(
        jnp.int32, wide, 1
    ) // SUB
    spread = jnp.where(spread, 1.0, 0.0).astype(jnp.bfloat16)
    wide_slot = dot(slot.T.astype(jnp.bfloat16), spread)
    wide_share = dot(share.T.astype(jnp.bfloat16), spread)
    place = lax.broadcasted_iota(jnp.int32, wide_slot.shape, 1) % SUB
    for kind in range(4):
        hit = wide_slot == slot_of(place, kind).astype(jnp.float32)
        blend_ref[kind] = jnp.where(hit, wide_share, 0.0).astype(jnp.bfloat16)


def project_body(
    heads_ref,
    stream_ref,
    weight_ref,
    gain_ref,
    ids_ref,
    score_ref,
    first_ref,
    out_ref,
    blend_ref,
    pick_ref,
    *,
    dp_count,
):
    heads = heads_ref.shape[0]
    experts = out_ref.shape[0]
    attended = jnp.concatenate([heads_ref[h] for h in range(heads)], axis=1)
    projected = dot(attended, weight_ref[...])
    route_into(ids_ref, score_ref, pick_ref, blend_ref, dp_count)
    summed = deep_alpha * stream_ref[0].astype(jnp.float32) + projected
    first = layer_norm(summed, gain_ref[...]).astype(jnp.bfloat16)
    first_ref[...] = first
    tail = first[:, MAIN * LANE :]
    for p in range(3):
        kept = [first[:, (3 * q + p) * LANE : (3 * q + p + 1) * LANE] for q in range(TAIL)]
        both = jnp.concatenate([jnp.concatenate(kept, axis=1), tail], axis=0)
        lhs = jnp.concatenate([pick_ref[0], pick_ref[p + 1]], axis=1)
        rows = dot(lhs, both).astype(jnp.bfloat16)
        for q in range(TAIL):
            tile = rows[:, q * LANE : (q + 1) * LANE]
            out_ref[:, 3 * q + p] = tile.reshape(experts, SUB, LANE)


def project(heads, stream, weight, gain, ids, scores, experts, dp_count):
    rows, width = stream.shape[1:]
    return call(
        functools.partial(project_body, dp_count=dp_count),
        (
            jax.ShapeDtypeStruct((rows, width), jnp.bfloat16),
            jax.ShapeDtypeStruct((experts, MAIN, SUB, LANE), jnp.bfloat16),
            jax.ShapeDtypeStruct((4, rows, experts * SUB), jnp.bfloat16),
        ),
        36,
        scratch_shapes=[pltpu.VMEM((4, experts * SUB, rows), jnp.bfloat16)],
    )(heads, stream, weight, gain, ids, scores)


def expert_body(in_ref, gate_ref, up_ref, down_ref, out_ref):
    groups = in_ref.shape[0]
    rows = groups * SUB
    units = gate_ref.shape[2]
    place = lax.broadcasted_iota(jnp.int32, (rows, LANE), 0) % SUB
    place = place.astype(jnp.int16)
    below = [place < jnp.int16(n) for n in (2, 4, SLOTS)]

    def moved(x, places):
        return pltpu.roll(x, places % rows, 0)

    def by_place(first, second, third, spare):
        rest = jnp.where(below[1], second, jnp.where(below[2], third, spare))
        return jnp.where(below[0], first, rest)

    came = [[in_ref[:, i, t].reshape(rows, LANE) for t in range(MAIN)] for i in range(4)]
    x = []
    for i in range(3):
        blocks = [
            jnp.where(below[2], came[i][t], moved(came[3][t], SLOTS - 2 * i)) for t in range(MAIN)
        ]
        for q in range(TAIL):
            own = [moved(came[i][3 * q + p], 2 * p - SLOTS) for p in range(3)]
            blocks.append(by_place(*own, came[3][3 * q + i]))
        x.append(jnp.concatenate(blocks, axis=1))
    x = jnp.concatenate(x, axis=0)
    hidden = []
    for lo in range(0, units, units // 2):
        half = slice(lo, lo + units // 2)
        gate_act = jnp.minimum(dot(x, gate_ref[0, :, half]), clamp_limit)
        up_act = jnp.clip(dot(x, up_ref[0, :, half]), -clamp_limit, clamp_limit)
        act = gate_act * jax.nn.sigmoid(swish_alpha * gate_act) * (up_act + 1.0)
        hidden.append(act.astype(jnp.bfloat16))
    hidden = jnp.concatenate(hidden, axis=1)
    y_tail = dot(hidden, down_ref[0, :, MAIN * LANE :]).astype(jnp.bfloat16)

    def part(y, i, c):
        return y[i * rows : (i + 1) * rows, c * LANE : (c + 1) * LANE]

    for first in range(0, MAIN, TAIL):
        y = dot(hidden, down_ref[0, :, first * LANE : (first + TAIL) * LANE])
        y = y.astype(jnp.bfloat16)
        for c in range(TAIL):
            t = first + c
            q, p = t // 3, t % 3
            tiles = [
                jnp.where(below[2], part(y, i, c), moved(part(y_tail, i, q), SLOTS - 2 * p))
                for i in range(3)
            ]
            lent = [moved(part(y, i, c), 2 * i - SLOTS) for i in range(3)]
            tiles.append(by_place(*lent, part(y_tail, p, q)))
            for i, tile in enumerate(tiles):
                out_ref[:, i, t] = tile.reshape(groups, SUB, LANE)


def expert(arrived, gate, up, down):
    sources, step = arrived.shape[0], 64
    fours = arrived.reshape(sources // 4, 4, *arrived.shape[1:])
    block = pl.BlockSpec((step // 4, *fours.shape[1:]), lambda i: (i, 0, 0, 0, 0))
    whole = [pl.BlockSpec(w.shape, lambda i: (0, 0, 0)) for w in (gate, up, down)]
    return call(
        expert_body,
        jax.ShapeDtypeStruct(fours.shape, fours.dtype),
        30,
        grid=(sources // step,),
        in_specs=[block] + whole,
        out_specs=block,
    )(fours, gate, up, down).reshape(arrived.shape)


def combine_body(in_ref, blend_ref, first_ref, gain_ref, out_ref):
    experts = in_ref.shape[0]
    tail = None
    blocks = [None] * MAIN
    for p in range(3):
        rows = [in_ref[:, 3 * q + p].reshape(experts * SUB, LANE) for q in range(TAIL)]
        both = jnp.concatenate([blend_ref[0], blend_ref[p + 1]], axis=0)
        mixed = dot(both, jnp.concatenate(rows, axis=1))
        count = blend_ref.shape[1]
        for q in range(TAIL):
            blocks[3 * q + p] = mixed[:count, q * LANE : (q + 1) * LANE]
        tail = mixed[count:] if tail is None else tail + mixed[count:]
    mixture = jnp.concatenate(blocks + [tail], axis=1)
    summed = deep_alpha * first_ref[...].astype(jnp.float32) + mixture
    out_ref[0] = layer_norm(summed, gain_ref[...]).astype(jnp.bfloat16)


def combine(returned, blend, first, gain):
    return call(
        combine_body,
        jax.ShapeDtypeStruct((1, *first.shape), jnp.bfloat16),
        36,
    )(returned, blend, first, gain)


def exchange(x, axes):
    return lax.all_to_all(x, axes, split_axis=0, concat_axis=0, tiled=True)


def shards(
    stream,
    query_rows,
    key_rows,
    value_rows,
    forget_sums,
    out_weight,
    first_gain,
    expert_ids,
    route_scores,
    gate_weight,
    up_weight,
    down_weight,
    second_gain,
):
    experts = lax.axis_size(SP_DP)
    qkv = exchange(pack(query_rows, key_rows, value_rows), SP)
    attended, near_weight = attend(qkv, forget_sums[0], out_weight)
    heads = exchange(attended, SP)
    first, outgoing, blend = project(
        heads,
        stream,
        near_weight,
        first_gain[None],
        expert_ids.transpose(0, 2, 1),
        route_scores.transpose(0, 2, 1),
        experts,
        lax.axis_size("dp"),
    )
    arrived = exchange(outgoing, DP_SP)
    finished = expert(arrived, gate_weight, up_weight, down_weight)
    returned = exchange(finished, DP_SP)
    return combine(returned, blend, first, second_gain[None])


def solution(mesh):
    finer = Mesh(mesh.devices.reshape(4, 4, mesh.shape["dp"]), ("sp_0", "sp_1", "dp"))
    rows = P("dp", SP, None)
    own = P(SP_DP, None, None)
    placed = (rows,) * 5 + (P(), P(), rows, rows, own, own, own, P())
    return jax.shard_map(shards, mesh=finer, in_specs=placed, out_specs=rows, check_vma=False)
```

```python
import functools

import jax
import jax.numpy as jnp
from jax import lax
from jax.experimental import pallas as pl
from jax.experimental.pallas import tpu as pltpu
from jax.sharding import Mesh
from jax.sharding import PartitionSpec as P

SP = ("sp_0", "sp_1")
DP = ("x_1", "x_0", "core")
SP_DP = SP + DP
DP_SP = ("x_0", "x_1", "core") + SP

deep_alpha = 8.0**0.25
clamp_limit = 7.0
swish_alpha = 1.702
norm_eps = 1e-05
mask_fill = -1e30
log2_e = 1.4426950408889634

LANE = 128
SUB = 8
SLOTS = 6
MAIN = 12
TAIL = 4
MIB = 1 << 20


def call(body, out_shape, vmem_mib, **kwargs):
    return pl.pallas_call(
        body,
        out_shape=out_shape,
        compiler_params=pltpu.CompilerParams(vmem_limit_bytes=vmem_mib * MIB),
        **kwargs,
    )


def dot(a, b, dims=((1,), (0,))):
    return lax.dot_general(a, b, (dims, ((), ())), preferred_element_type=jnp.float32)


def layer_norm(summed, gain_row):
    centre = jnp.mean(summed, axis=-1, keepdims=True)
    centred = summed - centre
    spread = jnp.mean(jnp.square(centred), axis=-1, keepdims=True)
    return centred * lax.rsqrt(spread + norm_eps) * gain_row


def in_hbm(*arrays):
    return tuple(pltpu.with_memory_space_constraint(a, pltpu.HBM) for a in arrays)


def pack_body(q_ref, k_ref, v_ref, out_ref, land_ref, sems):
    copies = [
        pltpu.make_async_copy(ref.at[0], land_ref.at[n], sems.at[n])
        for n, ref in enumerate((q_ref, k_ref, v_ref))
    ]
    for copy in copies:
        copy.start()
    for n, copy in enumerate(copies):
        copy.wait()
        for h in range(out_ref.shape[0]):
            out_ref[h, n] = land_ref[n, :, h * LANE : (h + 1) * LANE]


def pack(q, k, v):
    rows, width = q.shape[1:]
    return call(
        pack_body,
        pltpu.VMEM((width // LANE, 3, rows, LANE), q.dtype),
        8,
        in_specs=[pl.BlockSpec(memory_space=pltpu.HBM)] * 3,
        out_specs=pl.BlockSpec(memory_space=pltpu.VMEM),
        scratch_shapes=[
            pltpu.VMEM((3, rows, width), q.dtype),
            pltpu.SemaphoreType.DMA((3,)),
        ],
    )(*in_hbm(q, k, v))


def attend_body(qkv_ref, gate_ref, weight_ref, out_ref, near_ref, score_ref, sem):
    brought = pltpu.make_async_copy(weight_ref, near_ref, sem)
    brought.start()
    parts, _, rows, size = qkv_ref.shape
    pair = 2
    block = pair * rows
    scale = size ** (-0.5) * log2_e

    def part(j, n):
        return qkv_ref[pair * j : pair * (j + 1), n].reshape(block, size)

    def score_rows(b):
        q = part(b, 0)
        base = gate_ref[:, block * b : block * b + 1]
        top = jnp.full((block, LANE), mask_fill, jnp.float32)
        for j in range(b + 1):
            bias = (gate_ref[:, block * j : block * (j + 1)] - base) * log2_e
            s = dot(q, part(j, 1), ((1,), (1,))) * scale - bias
            if j == b:
                row = lax.broadcasted_iota(jnp.int32, s.shape, 0)
                col = lax.broadcasted_iota(jnp.int32, s.shape, 1)
                s = jnp.where(row >= col, s, mask_fill)
            score_ref[b % 2, :, block * j : block * (j + 1)] = s
            for c in range(block // LANE):
                top = jnp.maximum(top, s[:, c * LANE : (c + 1) * LANE])
        return jnp.max(top, axis=1, keepdims=True)

    def blend_rows(b, row_max):
        total = jnp.zeros((block, LANE), jnp.float32)
        blended = jnp.zeros((block, size), jnp.float32)
        for j in range(b + 1):
            w = jnp.exp2(score_ref[b % 2, :, block * j : block * (j + 1)] - row_max)
            for c in range(block // LANE):
                total = total + w[:, c * LANE : (c + 1) * LANE]
            blended = blended + dot(w.astype(jnp.bfloat16), part(j, 2))
        row_total = jnp.sum(total, axis=1, keepdims=True)
        done = (blended / row_total).astype(jnp.bfloat16)
        out_ref[pair * b : pair * (b + 1)] = done.reshape(pair, rows, size)

    last = parts // pair - 1
    row_max = score_rows(last)
    for b in range(last, -1, -1):
        ahead = score_rows(b - 1) if b > 0 else None
        blend_rows(b, row_max)
        row_max = ahead
    brought.wait()


def attend(qkv, gates, weight):
    parts, _, rows, size = qkv.shape
    near = pl.BlockSpec(memory_space=pltpu.VMEM)
    return call(
        attend_body,
        (
            jax.ShapeDtypeStruct((parts, rows, size), qkv.dtype),
            pltpu.VMEM(weight.shape, weight.dtype),
        ),
        20,
        in_specs=[near, near, pl.BlockSpec(memory_space=pltpu.HBM)],
        out_specs=(near, near),
        scratch_shapes=[
            pltpu.VMEM((2, 2 * rows, parts * rows), jnp.float32),
            pltpu.SemaphoreType.DMA,
        ],
    )(qkv, gates, *in_hbm(weight))


def slot_of(place, kind):
    if kind == 0:
        return jnp.where(place < SLOTS, place, -2)
    return jnp.where(place >= SLOTS, place - SLOTS + 2 * (kind - 1), -2)


def route_into(ids_ref, score_ref, pick_ref, blend_ref, dp_count):
    top_k, rows = ids_ref.shape[1:]
    experts = pick_ref.shape[1] // SUB
    turn = lax.broadcasted_iota(jnp.int32, (experts, rows), 0)
    sp_count = experts // dp_count
    outer = turn // sp_count
    quarter = dp_count // 4
    x_0, x_1 = outer // (2 * quarter), outer // quarter % 2
    expert = turn % sp_count * dp_count + (2 * x_1 + x_0) * quarter + outer % quarter
    scores = score_ref[0]
    raised = jnp.exp(scores - jnp.max(scores, axis=0, keepdims=True))
    shares = raised / jnp.sum(raised, axis=0, keepdims=True)
    named = jnp.zeros((experts, rows), jnp.float32)
    share = jnp.zeros((experts, rows), jnp.float32)
    for k in range(top_k):
        hit = ids_ref[0, k : k + 1] == expert
        named = jnp.where(hit, 1.0, named)
        share = jnp.where(hit, shares[k : k + 1], share)
    earlier = lax.broadcasted_iota(jnp.int32, (rows, rows), 0) < lax.broadcasted_iota(
        jnp.int32, (rows, rows), 1
    )
    rank = dot(named.astype(jnp.bfloat16), jnp.where(earlier, 1.0, 0.0).astype(jnp.bfloat16))
    slot = jnp.where(named > 0.0, rank, -1.0)
    by_expert = jnp.broadcast_to(slot[:, None, :], (experts, SUB, rows))
    place = lax.broadcasted_iota(jnp.int32, (experts, SUB, rows), 1)
    for kind in range(4):
        hit = by_expert == slot_of(place, kind).astype(jnp.float32)
        pick = jnp.where(hit, 1.0, 0.0).reshape(experts * SUB, rows).astype(jnp.bfloat16)
        pick_ref[kind] = pick
    wide = (experts, experts * SUB)
    spread = lax.broadcasted_iota(jnp.int32, wide, 0) == lax.broadcasted_iota(
        jnp.int32, wide, 1
    ) // SUB
    spread = jnp.where(spread, 1.0, 0.0).astype(jnp.bfloat16)
    wide_slot = dot(slot.T.astype(jnp.bfloat16), spread)
    wide_share = dot(share.T.astype(jnp.bfloat16), spread)
    place = lax.broadcasted_iota(jnp.int32, wide_slot.shape, 1) % SUB
    for kind in range(4):
        hit = wide_slot == slot_of(place, kind).astype(jnp.float32)
        blend_ref[kind] = jnp.where(hit, wide_share, 0.0).astype(jnp.bfloat16)


def project_body(
    heads_ref,
    stream_ref,
    weight_ref,
    gain_ref,
    ids_ref,
    score_ref,
    first_ref,
    out_ref,
    blend_ref,
    pick_ref,
    *,
    dp_count,
):
    heads = heads_ref.shape[0]
    experts = out_ref.shape[0]
    attended = jnp.concatenate([heads_ref[h] for h in range(heads)], axis=1)
    projected = dot(attended, weight_ref[...])
    route_into(ids_ref, score_ref, pick_ref, blend_ref, dp_count)
    summed = deep_alpha * stream_ref[0].astype(jnp.float32) + projected
    first = layer_norm(summed, gain_ref[...]).astype(jnp.bfloat16)
    first_ref[...] = first
    tail = first[:, MAIN * LANE :]
    for p in range(3):
        kept = [first[:, (3 * q + p) * LANE : (3 * q + p + 1) * LANE] for q in range(TAIL)]
        both = jnp.concatenate([jnp.concatenate(kept, axis=1), tail], axis=0)
        lhs = jnp.concatenate([pick_ref[0], pick_ref[p + 1]], axis=1)
        rows = dot(lhs, both).astype(jnp.bfloat16)
        for q in range(TAIL):
            tile = rows[:, q * LANE : (q + 1) * LANE]
            out_ref[:, 3 * q + p] = tile.reshape(experts, SUB, LANE)


def project(heads, stream, weight, gain, ids, scores, experts, dp_count):
    rows, width = stream.shape[1:]
    return call(
        functools.partial(project_body, dp_count=dp_count),
        (
            jax.ShapeDtypeStruct((rows, width), jnp.bfloat16),
            jax.ShapeDtypeStruct((experts, MAIN, SUB, LANE), jnp.bfloat16),
            jax.ShapeDtypeStruct((4, rows, experts * SUB), jnp.bfloat16),
        ),
        36,
        scratch_shapes=[pltpu.VMEM((4, experts * SUB, rows), jnp.bfloat16)],
    )(heads, stream, weight, gain, ids, scores)


def expert_body(in_ref, gate_ref, up_ref, down_ref, out_ref):
    groups = in_ref.shape[0]
    rows = groups * SUB
    units = gate_ref.shape[2]
    place = lax.broadcasted_iota(jnp.int32, (rows, LANE), 0) % SUB
    place = place.astype(jnp.int16)
    below = [place < jnp.int16(n) for n in (2, 4, SLOTS)]

    def moved(x, places):
        return pltpu.roll(x, places % rows, 0)

    def by_place(first, second, third, spare):
        rest = jnp.where(below[1], second, jnp.where(below[2], third, spare))
        return jnp.where(below[0], first, rest)

    came = [[in_ref[:, i, t].reshape(rows, LANE) for t in range(MAIN)] for i in range(4)]
    x = []
    for i in range(3):
        blocks = [
            jnp.where(below[2], came[i][t], moved(came[3][t], SLOTS - 2 * i)) for t in range(MAIN)
        ]
        for q in range(TAIL):
            own = [moved(came[i][3 * q + p], 2 * p - SLOTS) for p in range(3)]
            blocks.append(by_place(*own, came[3][3 * q + i]))
        x.append(jnp.concatenate(blocks, axis=1))
    x = jnp.concatenate(x, axis=0)
    hidden = []
    for lo in range(0, units, units // 2):
        half = slice(lo, lo + units // 2)
        gate_act = jnp.minimum(dot(x, gate_ref[0, :, half]), clamp_limit)
        up_act = jnp.clip(dot(x, up_ref[0, :, half]), -clamp_limit, clamp_limit)
        act = gate_act * jax.nn.sigmoid(swish_alpha * gate_act) * (up_act + 1.0)
        hidden.append(act.astype(jnp.bfloat16))
    hidden = jnp.concatenate(hidden, axis=1)
    y_tail = dot(hidden, down_ref[0, :, MAIN * LANE :]).astype(jnp.bfloat16)

    def part(y, i, c):
        return y[i * rows : (i + 1) * rows, c * LANE : (c + 1) * LANE]

    step = MAIN // 2
    for first in range(0, MAIN, step):
        y = dot(hidden, down_ref[0, :, first * LANE : (first + step) * LANE])
        y = y.astype(jnp.bfloat16)
        for c in range(step):
            t = first + c
            q, p = t // 3, t % 3
            tiles = [
                jnp.where(below[2], part(y, i, c), moved(part(y_tail, i, q), SLOTS - 2 * p))
                for i in range(3)
            ]
            lent = [moved(part(y, i, c), 2 * i - SLOTS) for i in range(3)]
            tiles.append(by_place(*lent, part(y_tail, p, q)))
            for i, tile in enumerate(tiles):
                out_ref[:, i, t] = tile.reshape(groups, SUB, LANE)


def expert(arrived, gate, up, down):
    sources, step = arrived.shape[0], 64
    fours = arrived.reshape(sources // 4, 4, *arrived.shape[1:])
    block = pl.BlockSpec((step // 4, *fours.shape[1:]), lambda i: (i, 0, 0, 0, 0))
    whole = [pl.BlockSpec(w.shape, lambda i: (0, 0, 0)) for w in (gate, up, down)]
    return call(
        expert_body,
        jax.ShapeDtypeStruct(fours.shape, fours.dtype),
        30,
        grid=(sources // step,),
        in_specs=[block] + whole,
        out_specs=block,
    )(fours, gate, up, down).reshape(arrived.shape)


def combine_body(in_ref, blend_ref, first_ref, gain_ref, out_ref):
    experts = in_ref.shape[0]
    tail = None
    blocks = [None] * MAIN
    for p in range(3):
        rows = [in_ref[:, 3 * q + p].reshape(experts * SUB, LANE) for q in range(TAIL)]
        both = jnp.concatenate([blend_ref[0], blend_ref[p + 1]], axis=0)
        mixed = dot(both, jnp.concatenate(rows, axis=1))
        count = blend_ref.shape[1]
        for q in range(TAIL):
            blocks[3 * q + p] = mixed[:count, q * LANE : (q + 1) * LANE]
        tail = mixed[count:] if tail is None else tail + mixed[count:]
    mixture = jnp.concatenate(blocks + [tail], axis=1)
    summed = deep_alpha * first_ref[...].astype(jnp.float32) + mixture
    out_ref[0] = layer_norm(summed, gain_ref[...]).astype(jnp.bfloat16)


def combine(returned, blend, first, gain):
    return call(
        combine_body,
        jax.ShapeDtypeStruct((1, *first.shape), jnp.bfloat16),
        36,
    )(returned, blend, first, gain)


def exchange(x, axes):
    return lax.all_to_all(x, axes, split_axis=0, concat_axis=0, tiled=True)


def shards(
    stream,
    query_rows,
    key_rows,
    value_rows,
    forget_sums,
    out_weight,
    first_gain,
    expert_ids,
    route_scores,
    gate_weight,
    up_weight,
    down_weight,
    second_gain,
):
    experts = lax.axis_size(SP_DP)
    qkv = exchange(pack(query_rows, key_rows, value_rows), SP)
    attended, near_weight = attend(qkv, forget_sums[0], out_weight)
    heads = exchange(attended, SP)
    first, outgoing, blend = project(
        heads,
        stream,
        near_weight,
        first_gain[None],
        expert_ids.transpose(0, 2, 1),
        route_scores.transpose(0, 2, 1),
        experts,
        lax.axis_size(DP),
    )
    arrived = exchange(outgoing, DP_SP)
    finished = expert(arrived, gate_weight, up_weight, down_weight)
    returned = exchange(finished, DP_SP)
    return combine(returned, blend, first, second_gain[None])


def solution(mesh):
    finer = Mesh(mesh.devices.reshape(4, 4, 2, 2, 2), SP_DP)
    rows = P(DP, SP, None)
    own = P(SP_DP, None, None)
    placed = (rows,) * 5 + (P(), P(), rows, rows, own, own, own, P())
    return jax.shard_map(shards, mesh=finer, in_specs=placed, out_specs=rows, check_vma=False)
```

```python
import functools

import jax
import jax.numpy as jnp
from jax import lax
from jax.experimental import pallas as pl
from jax.experimental.pallas import tpu as pltpu
from jax.sharding import Mesh
from jax.sharding import PartitionSpec as P

SP = ("sp_0", "sp_1")
SP_DP = ("sp_0", "sp_1", "dp")
DP_SP = ("dp", "sp_0", "sp_1")

deep_alpha = 8.0**0.25
clamp_limit = 7.0
swish_alpha = 1.702
norm_eps = 1e-05
mask_fill = -1e30
log2_e = 1.4426950408889634

LANE = 128
SUB = 8
SLOTS = 6
MAIN = 12
TAIL = 4
MIB = 1 << 20


def call(body, out_shape, vmem_mib, **kwargs):
    return pl.pallas_call(
        body,
        out_shape=out_shape,
        compiler_params=pltpu.CompilerParams(vmem_limit_bytes=vmem_mib * MIB),
        **kwargs,
    )


def dot(a, b, dims=((1,), (0,))):
    return lax.dot_general(a, b, (dims, ((), ())), preferred_element_type=jnp.float32)


def layer_norm(summed, gain_row):
    centre = jnp.mean(summed, axis=-1, keepdims=True)
    centred = summed - centre
    spread = jnp.mean(jnp.square(centred), axis=-1, keepdims=True)
    return centred * lax.rsqrt(spread + norm_eps) * gain_row


def in_hbm(*arrays):
    return tuple(pltpu.with_memory_space_constraint(a, pltpu.HBM) for a in arrays)


def pack_body(q_ref, k_ref, v_ref, out_ref, land_ref, sems):
    copies = [
        pltpu.make_async_copy(ref.at[0], land_ref.at[n], sems.at[n])
        for n, ref in enumerate((q_ref, k_ref, v_ref))
    ]
    for copy in copies:
        copy.start()
    for n, copy in enumerate(copies):
        copy.wait()
        for h in range(out_ref.shape[0]):
            out_ref[h, n] = land_ref[n, :, h * LANE : (h + 1) * LANE]


def pack(q, k, v):
    rows, width = q.shape[1:]
    return call(
        pack_body,
        pltpu.VMEM((width // LANE, 3, rows, LANE), q.dtype),
        8,
        in_specs=[pl.BlockSpec(memory_space=pltpu.HBM)] * 3,
        out_specs=pl.BlockSpec(memory_space=pltpu.VMEM),
        scratch_shapes=[
            pltpu.VMEM((3, rows, width), q.dtype),
            pltpu.SemaphoreType.DMA((3,)),
        ],
    )(*in_hbm(q, k, v))


def attend_body(qkv_ref, gate_ref, weight_ref, out_ref, near_ref, score_ref, sem):
    brought = pltpu.make_async_copy(weight_ref, near_ref, sem)
    brought.start()
    parts, _, rows, size = qkv_ref.shape
    pair = 2
    block = pair * rows
    scale = size ** (-0.5) * log2_e

    def part(j, n):
        return qkv_ref[pair * j : pair * (j + 1), n].reshape(block, size)

    def score_rows(b):
        q = part(b, 0)
        base = gate_ref[:, block * b : block * b + 1]
        top = jnp.full((block, LANE), mask_fill, jnp.float32)
        for j in range(b + 1):
            bias = (gate_ref[:, block * j : block * (j + 1)] - base) * log2_e
            s = dot(q, part(j, 1), ((1,), (1,))) * scale - bias
            if j == b:
                row = lax.broadcasted_iota(jnp.int32, s.shape, 0)
                col = lax.broadcasted_iota(jnp.int32, s.shape, 1)
                s = jnp.where(row >= col, s, mask_fill)
            score_ref[b % 2, :, block * j : block * (j + 1)] = s
            for c in range(block // LANE):
                top = jnp.maximum(top, s[:, c * LANE : (c + 1) * LANE])
        return jnp.max(top, axis=1, keepdims=True)

    ones = jnp.ones((block, LANE), jnp.bfloat16)

    def blend_rows(b, row_max):
        blended = jnp.zeros((block, size + LANE), jnp.float32)
        for j in range(b + 1):
            w = jnp.exp2(score_ref[b % 2, :, block * j : block * (j + 1)] - row_max)
            sides = jnp.concatenate([part(j, 2), ones], axis=1)
            blended = blended + dot(w.astype(jnp.bfloat16), sides)
        done = (blended[:, :size] / blended[:, size:]).astype(jnp.bfloat16)
        out_ref[pair * b : pair * (b + 1)] = done.reshape(pair, rows, size)

    last = parts // pair - 1
    row_max = score_rows(last)
    for b in range(last, -1, -1):
        ahead = score_rows(b - 1) if b > 0 else None
        blend_rows(b, row_max)
        row_max = ahead
    brought.wait()


def attend(qkv, gates, weight):
    parts, _, rows, size = qkv.shape
    near = pl.BlockSpec(memory_space=pltpu.VMEM)
    return call(
        attend_body,
        (
            jax.ShapeDtypeStruct((parts, rows, size), qkv.dtype),
            pltpu.VMEM(weight.shape, weight.dtype),
        ),
        20,
        in_specs=[near, near, pl.BlockSpec(memory_space=pltpu.HBM)],
        out_specs=(near, near),
        scratch_shapes=[
            pltpu.VMEM((2, 2 * rows, parts * rows), jnp.float32),
            pltpu.SemaphoreType.DMA,
        ],
    )(qkv, gates, *in_hbm(weight))


def slot_of(place, kind):
    if kind == 0:
        return jnp.where(place < SLOTS, place, -2)
    return jnp.where(place >= SLOTS, place - SLOTS + 2 * (kind - 1), -2)


def route_into(ids_ref, score_ref, pick_ref, blend_ref, dp_count):
    top_k, rows = ids_ref.shape[1:]
    experts = pick_ref.shape[1] // SUB
    turn = lax.broadcasted_iota(jnp.int32, (experts, rows), 0)
    sp_count = experts // dp_count
    expert = turn % sp_count * dp_count + turn // sp_count
    scores = score_ref[0]
    raised = jnp.exp(scores - jnp.max(scores, axis=0, keepdims=True))
    shares = raised / jnp.sum(raised, axis=0, keepdims=True)
    named = jnp.zeros((experts, rows), jnp.float32)
    share = jnp.zeros((experts, rows), jnp.float32)
    for k in range(top_k):
        hit = ids_ref[0, k : k + 1] == expert
        named = jnp.where(hit, 1.0, named)
        share = jnp.where(hit, shares[k : k + 1], share)
    earlier = lax.broadcasted_iota(jnp.int32, (rows, rows), 0) < lax.broadcasted_iota(
        jnp.int32, (rows, rows), 1
    )
    rank = dot(named.astype(jnp.bfloat16), jnp.where(earlier, 1.0, 0.0).astype(jnp.bfloat16))
    slot = jnp.where(named > 0.0, rank, -1.0)
    by_expert = jnp.broadcast_to(slot[:, None, :], (experts, SUB, rows))
    place = lax.broadcasted_iota(jnp.int32, (experts, SUB, rows), 1)
    for kind in range(4):
        hit = by_expert == slot_of(place, kind).astype(jnp.float32)
        pick = jnp.where(hit, 1.0, 0.0).reshape(experts * SUB, rows).astype(jnp.bfloat16)
        pick_ref[kind] = pick
    wide = (experts, experts * SUB)
    spread = lax.broadcasted_iota(jnp.int32, wide, 0) == lax.broadcasted_iota(
        jnp.int32, wide, 1
    ) // SUB
    spread = jnp.where(spread, 1.0, 0.0).astype(jnp.bfloat16)
    wide_slot = dot(slot.T.astype(jnp.bfloat16), spread)
    wide_share = dot(share.T.astype(jnp.bfloat16), spread)
    place = lax.broadcasted_iota(jnp.int32, wide_slot.shape, 1) % SUB
    for kind in range(4):
        hit = wide_slot == slot_of(place, kind).astype(jnp.float32)
        blend_ref[kind] = jnp.where(hit, wide_share, 0.0).astype(jnp.bfloat16)


def project_body(
    heads_ref,
    stream_ref,
    weight_ref,
    gain_ref,
    ids_ref,
    score_ref,
    first_ref,
    out_ref,
    blend_ref,
    pick_ref,
    *,
    dp_count,
):
    heads = heads_ref.shape[0]
    experts = out_ref.shape[0]
    attended = jnp.concatenate([heads_ref[h] for h in range(heads)], axis=1)
    projected = dot(attended, weight_ref[...])
    route_into(ids_ref, score_ref, pick_ref, blend_ref, dp_count)
    summed = deep_alpha * stream_ref[0].astype(jnp.float32) + projected
    first = layer_norm(summed, gain_ref[...]).astype(jnp.bfloat16)
    first_ref[...] = first
    tail = first[:, MAIN * LANE :]
    for p in range(3):
        kept = [first[:, (3 * q + p) * LANE : (3 * q + p + 1) * LANE] for q in range(TAIL)]
        both = jnp.concatenate([jnp.concatenate(kept, axis=1), tail], axis=0)
        lhs = jnp.concatenate([pick_ref[0], pick_ref[p + 1]], axis=1)
        rows = dot(lhs, both).astype(jnp.bfloat16)
        for q in range(TAIL):
            tile = rows[:, q * LANE : (q + 1) * LANE]
            out_ref[:, 3 * q + p] = tile.reshape(experts, SUB, LANE)


def project(heads, stream, weight, gain, ids, scores, experts, dp_count):
    rows, width = stream.shape[1:]
    return call(
        functools.partial(project_body, dp_count=dp_count),
        (
            jax.ShapeDtypeStruct((rows, width), jnp.bfloat16),
            jax.ShapeDtypeStruct((experts, MAIN, SUB, LANE), jnp.bfloat16),
            jax.ShapeDtypeStruct((4, rows, experts * SUB), jnp.bfloat16),
        ),
        36,
        scratch_shapes=[pltpu.VMEM((4, experts * SUB, rows), jnp.bfloat16)],
    )(heads, stream, weight, gain, ids, scores)


def expert_body(in_ref, gate_ref, up_ref, down_ref, out_ref):
    groups = in_ref.shape[0]
    rows = groups * SUB
    units = gate_ref.shape[2]
    place = lax.broadcasted_iota(jnp.int32, (rows, LANE), 0) % SUB
    place = place.astype(jnp.int16)
    below = [place < jnp.int16(n) for n in (2, 4, SLOTS)]

    def moved(x, places):
        return pltpu.roll(x, places % rows, 0)

    def by_place(first, second, third, spare):
        rest = jnp.where(below[1], second, jnp.where(below[2], third, spare))
        return jnp.where(below[0], first, rest)

    came = [[in_ref[:, i, t].reshape(rows, LANE) for t in range(MAIN)] for i in range(4)]
    x = []
    for i in range(3):
        blocks = [
            jnp.where(below[2], came[i][t], moved(came[3][t], SLOTS - 2 * i)) for t in range(MAIN)
        ]
        for q in range(TAIL):
            own = [moved(came[i][3 * q + p], 2 * p - SLOTS) for p in range(3)]
            blocks.append(by_place(*own, came[3][3 * q + i]))
        x.append(jnp.concatenate(blocks, axis=1))
    x = jnp.concatenate(x, axis=0)
    hidden = []
    for lo in range(0, units, units // 2):
        half = slice(lo, lo + units // 2)
        gate_act = jnp.minimum(dot(x, gate_ref[0, :, half]), clamp_limit)
        up_act = jnp.clip(dot(x, up_ref[0, :, half]), -clamp_limit, clamp_limit)
        act = gate_act * jax.nn.sigmoid(swish_alpha * gate_act) * (up_act + 1.0)
        hidden.append(act.astype(jnp.bfloat16))
    hidden = jnp.concatenate(hidden, axis=1)
    y_tail = dot(hidden, down_ref[0, :, MAIN * LANE :]).astype(jnp.bfloat16)

    def part(y, i, c):
        return y[i * rows : (i + 1) * rows, c * LANE : (c + 1) * LANE]

    for first in range(0, MAIN, TAIL):
        y = dot(hidden, down_ref[0, :, first * LANE : (first + TAIL) * LANE])
        y = y.astype(jnp.bfloat16)
        for c in range(TAIL):
            t = first + c
            q, p = t // 3, t % 3
            tiles = [
                jnp.where(below[2], part(y, i, c), moved(part(y_tail, i, q), SLOTS - 2 * p))
                for i in range(3)
            ]
            lent = [moved(part(y, i, c), 2 * i - SLOTS) for i in range(3)]
            tiles.append(by_place(*lent, part(y_tail, p, q)))
            for i, tile in enumerate(tiles):
                out_ref[:, i, t] = tile.reshape(groups, SUB, LANE)


def expert(arrived, gate, up, down):
    sources, step = arrived.shape[0], 64
    fours = arrived.reshape(sources // 4, 4, *arrived.shape[1:])
    block = pl.BlockSpec((step // 4, *fours.shape[1:]), lambda i: (i, 0, 0, 0, 0))
    whole = [pl.BlockSpec(w.shape, lambda i: (0, 0, 0)) for w in (gate, up, down)]
    return call(
        expert_body,
        jax.ShapeDtypeStruct(fours.shape, fours.dtype),
        30,
        grid=(sources // step,),
        in_specs=[block] + whole,
        out_specs=block,
    )(fours, gate, up, down).reshape(arrived.shape)


def combine_body(in_ref, blend_ref, first_ref, gain_ref, out_ref):
    experts = in_ref.shape[0]
    tail = None
    blocks = [None] * MAIN
    for p in range(3):
        rows = [in_ref[:, 3 * q + p].reshape(experts * SUB, LANE) for q in range(TAIL)]
        both = jnp.concatenate([blend_ref[0], blend_ref[p + 1]], axis=0)
        mixed = dot(both, jnp.concatenate(rows, axis=1))
        count = blend_ref.shape[1]
        for q in range(TAIL):
            blocks[3 * q + p] = mixed[:count, q * LANE : (q + 1) * LANE]
        tail = mixed[count:] if tail is None else tail + mixed[count:]
    mixture = jnp.concatenate(blocks + [tail], axis=1)
    summed = deep_alpha * first_ref[...].astype(jnp.float32) + mixture
    out_ref[0] = layer_norm(summed, gain_ref[...]).astype(jnp.bfloat16)


def combine(returned, blend, first, gain):
    return call(
        combine_body,
        jax.ShapeDtypeStruct((1, *first.shape), jnp.bfloat16),
        36,
    )(returned, blend, first, gain)


def exchange(x, axes):
    return lax.all_to_all(x, axes, split_axis=0, concat_axis=0, tiled=True)


def shards(
    stream,
    query_rows,
    key_rows,
    value_rows,
    forget_sums,
    out_weight,
    first_gain,
    expert_ids,
    route_scores,
    gate_weight,
    up_weight,
    down_weight,
    second_gain,
):
    experts = lax.axis_size(SP_DP)
    qkv = exchange(pack(query_rows, key_rows, value_rows), SP)
    attended, near_weight = attend(qkv, forget_sums[0], out_weight)
    heads = exchange(attended, SP)
    first, outgoing, blend = project(
        heads,
        stream,
        near_weight,
        first_gain[None],
        expert_ids.transpose(0, 2, 1),
        route_scores.transpose(0, 2, 1),
        experts,
        lax.axis_size("dp"),
    )
    arrived = exchange(outgoing, DP_SP)
    finished = expert(arrived, gate_weight, up_weight, down_weight)
    returned = exchange(finished, DP_SP)
    return combine(returned, blend, first, second_gain[None])


def solution(mesh):
    finer = Mesh(mesh.devices.reshape(4, 4, mesh.shape["dp"]), ("sp_0", "sp_1", "dp"))
    rows = P("dp", SP, None)
    own = P(SP_DP, None, None)
    placed = (rows,) * 5 + (P(), P(), rows, rows, own, own, own, P())
    return jax.shard_map(shards, mesh=finer, in_specs=placed, out_specs=rows, check_vma=False)
```
